32 devices in a mesh: sp: 32 (over z, y, x, core), tp: 1.
Axes of the slice: x: 2, y: 2, z: 4, core: 2. Of those that a mesh axis runs over, the one named last changes fastest.
Arguments:
- queries: bfloat16 [8192, 1024], P('sp', 'tp'), may hold values from -30 to 30
- keys: bfloat16 [8192, 256], P('sp', 'tp'), may hold values from -30 to 30
- values: bfloat16 [8192, 256], P('sp', 'tp'), may hold values from -20 to 20
- gate_totals: float32 [8192, 16], P('sp', 'tp'), may hold values from -8192 to 0, as said below
- documents: int32 [8192], P('sp'), may hold values from 0 to 1, never falling along the last dimension, each value on 1 to 6144 neighbouring positions
- stream: bfloat16 [8192, 2048], P(('sp', 'tp')), may hold values from -3 to 3
- out_weight: bfloat16 [1024, 2048], replicated, may hold values from -0.1875 to 0.1875
- norm_gain: float32 [2048], replicated, may hold values from 0.1 to 1.9
- routes: int32 [8192, 2], P(('sp', 'tp')), may hold values from 0 to 31, all different within a row; in each aligned block of 256 rows (0 to 255, 256 to 511, ...) at most 32 rows name the same one
- route_weights: float32 [8192, 2], P(('sp', 'tp')), may hold values from 0.2 to 1
- expert_gate: bfloat16 [32, 2048, 1024], P('sp', None, 'tp'), may hold values from -0.125 to 0.125
- expert_up: bfloat16 [32, 2048, 1024], P('sp', None, 'tp'), may hold values from -0.125 to 0.125
- expert_down: bfloat16 [32, 1024, 2048], P('sp', 'tp'), may hold values from -0.1875 to 0.1875
Outputs:
- output: bfloat16 [8192, 2048], P(('sp', 'tp'))
The draws below stay inside these ranges and needn't reach their ends.
Inputs may be any that keep to these rules, and one draw needn't show every extreme that they name: `gate_totals`: along positions it never rises, for every head. `routes`: in each aligned block of rows held by one device, no expert is named by more than 32 rows.
All inputs are finite; a program needn't handle non-finite values.
Results may differ from the reference program's by a relative error of at most 0.014.
Values may be sent and summed in bfloat16 or wider, within the bound.
A program may use at most 128 MiB of HBM per device.

```python
import math
import jax
import jax.numpy as jnp
import numpy as np
from jax import lax

D = 2048
QUERY_HEAD_COUNT = 16
KV_HEADS = 4
HD = 64
FF = 1024
TOP = 2
DOCS = 2
TOK_DEV = 256
SEQUENCE_TOKENS = 8192
EXPERTS = 32
CAP = 32
DOC_MOST = 6144
N_SP = 32
N_TP = 1


def draw_keys(key, part):
    base = jax.random.normal(jax.random.fold_in(key, 2), (SEQUENCE_TOKENS, KV_HEADS, HD), jnp.float32)
    return base.reshape(SEQUENCE_TOKENS, KV_HEADS * HD).astype(jnp.bfloat16)


def draw_queries(key, part):
    group = QUERY_HEAD_COUNT // KV_HEADS
    base = jax.random.normal(jax.random.fold_in(key, 1), (SEQUENCE_TOKENS, KV_HEADS, group, HD), jnp.float32)
    return base.reshape(SEQUENCE_TOKENS, QUERY_HEAD_COUNT * HD).astype(jnp.bfloat16)


def draw_gate_totals(key, part):
    ranking = jax.random.permutation(jax.random.fold_in(key, 21), QUERY_HEAD_COUNT)
    faster_variant = ranking < QUERY_HEAD_COUNT // 2
    slow_total = jax.random.uniform(jax.random.fold_in(key, 22), (QUERY_HEAD_COUNT,), jnp.float32, 0.15, 0.5)
    quick_rate = 1.0 / jax.random.uniform(jax.random.fold_in(key, 23), (QUERY_HEAD_COUNT,), jnp.float32, 30.0, 60.0)
    decay_speed = jnp.where(faster_variant, quick_rate, slow_total / SEQUENCE_TOKENS)
    machine_multiplier = jnp.exp(jax.random.uniform(jax.random.fold_in(key, 24), (SEQUENCE_TOKENS // TOK_DEV, 1), jnp.float32, -0.7, 0.7))
    machine_multiplier = jnp.repeat(machine_multiplier, TOK_DEV, axis=0)
    coarse_estimate = jax.random.uniform(jax.random.fold_in(key, 25), (SEQUENCE_TOKENS, QUERY_HEAD_COUNT), jnp.float32, 0.4, 1.6)
    cluster_positions = jax.random.randint(jax.random.fold_in(key, 26), (2, QUERY_HEAD_COUNT), 0, SEQUENCE_TOKENS)
    cluster_dropout = jnp.log(jax.random.uniform(jax.random.fold_in(key, 27), (2, QUERY_HEAD_COUNT), jnp.float32, 0.55, 0.8))
    locations = jnp.arange(SEQUENCE_TOKENS, dtype=jnp.int32)[:, None]
    token_clusters = jnp.where(locations == cluster_positions[0][None, :], cluster_dropout[0][None, :], 0.0)
    token_clusters = token_clusters + jnp.where(locations == cluster_positions[1][None, :], cluster_dropout[1][None, :], 0.0)
    logarithm_gate = -decay_speed[None, :] * machine_multiplier * coarse_estimate + jnp.where(faster_variant[None, :], 0.0, token_clusters)
    return jnp.cumsum(logarithm_gate, axis=0).astype(jnp.float32)


def shard_levels(rng, shape, shards, smallest, top_value):
    loudness = 1.0
    for axis_at, parts in shards:
        heights = jax.random.uniform(jax.random.fold_in(jax.random.fold_in(rng, 6), axis_at), (parts,), jnp.float32, smallest / len(shards), top_value / len(shards))
        loudness = loudness * jnp.repeat(jnp.exp(heights), shape[axis_at] // parts).reshape((-1,) + (1,) * (len(shape) - 1 - axis_at))
    return loudness


def length_profile(count, total, bound, slope):
    loads = [(1 << 20) // math.isqrt(grade ** slope) + 1 for grade in range(2, count + 1)]
    rest, counts = total - bound - (count - 1), [1] * (count - 1)
    while rest > 0:
        free = [i for i in range(count - 1) if counts[i] < bound]
        whole, remaining = sum([loads[i] for i in free]), rest
        for i in free:
            extra = min(bound - counts[i], max(1, remaining * loads[i] // whole), rest)
            counts[i] = counts[i] + extra
            rest = rest - extra
    return np.array([bound] + counts)


def ragged_sizes(stream_key, amount, total, most, slope):
    if amount == 2:
        one = jax.random.randint(stream_key, (), max(1, total - most), min(most, total - 1) + 1)
        return jnp.stack([one, total - one])
    tallies = jnp.asarray(length_profile(amount, total, most, slope), jnp.int32)
    twos = (amount - 1) // 2
    donor, receiver = tallies[1:1 + 2 * twos:2], tallies[2:2 + 2 * twos:2]
    slack = jnp.minimum(donor - 1, most - receiver)
    shifted = jax.random.randint(jax.random.fold_in(stream_key, 1), (twos,), 0, 1 << 20) % (slack + 1)
    tallies = tallies.at[1:1 + 2 * twos:2].set(donor - shifted).at[2:2 + 2 * twos:2].set(receiver + shifted)
    return tallies[jax.random.permutation(jax.random.fold_in(stream_key, 2), amount)]


def assign_block(own_key, own, number, rows, amount, top, most, slope):
    order = jax.random.permutation(own_key, amount)
    crowded, usual = portions_of(amount, rows * top, most, slope, True), portions_of(amount, rows * top, most, slope, False)
    places = jnp.arange(amount)

    def named(sizes, offset_by):
        used = int((sizes > 0).sum())
        fixed = max(1, used // 4)
        passed = fixed + (places - fixed + offset_by * (used - fixed)) % max(1, amount - fixed)
        return jnp.zeros((amount,), jnp.int32).at[order[jnp.where(places < fixed, places, passed)]].set(jnp.asarray(sizes, jnp.int32))

    sizes = jnp.where(number % 4 == 0, named(crowded, number // 4), named(usual, number - number // 4 - 1))
    mixed = jax.random.permutation(jax.random.fold_in(own, 3), amount)
    donor, taker = mixed[0:amount // 2 * 2:2], mixed[1:amount // 2 * 2:2]
    slack = jnp.minimum(sizes[donor] - 1, most - sizes[taker]) // 2
    slack = jnp.where((donor == order[0]) | (taker == order[0]) | (sizes[taker] == 0), 0, jnp.maximum(slack, 0))
    passed = jax.random.randint(jax.random.fold_in(own, 4), (amount // 2,), 0, 1 << 20) % (slack + 1)
    sizes = sizes.at[donor].add(-passed).at[taker].add(passed)
    labels = jnp.searchsorted(jnp.cumsum(sizes), jnp.arange(rows * top), side="right").astype(jnp.int32)
    table = labels.reshape(top, rows).T
    table = table[jax.random.permutation(jax.random.fold_in(own, 1), rows)]
    offset_by = jax.random.randint(jax.random.fold_in(own, 2), (rows, 1), 0, top)
    return jnp.take_along_axis(table, (jnp.arange(top)[None, :] + offset_by) % top, axis=1)


def portions_of(amount, total, bound, slope, full):
    weights = [(1 << 20) // math.isqrt(standing ** slope) + 1 for standing in range(1, amount + 1)]
    largest = bound if full else min(bound, max(-(-total // amount), total * weights[0] // sum(weights)))
    least = 1 if total - largest >= amount - 1 else 0
    counts, spare = [largest] + [least] * (amount - 1), total - largest - least * (amount - 1)
    while spare > 0:
        free = [i for i in range(1, amount) if counts[i] < largest] or [i for i in range(1, amount) if counts[i] < bound]
        whole, budget = sum([weights[i] for i in free]), spare
        for i in free:
            more = min(bound - counts[i], max(1, budget * weights[i] // whole), spare)
            counts[i] = counts[i] + more
            spare = spare - more
    return np.array(counts)


def normal_values(key, extent, deviation, reach, split=(), kind=jnp.bfloat16):
    values = jax.random.normal(key, extent, jnp.float32) * deviation
    if len(split) > 0:
        values = shard_levels(key, extent, split, -0.22, 0.18) * values
    return jnp.clip(values, min=-reach, max=reach).astype(kind)


def setup_inputs(seed: int = 0) -> dict:
    splits = jax.random.split(jax.random.key(seed), 14)
    queries = draw_queries(jax.random.fold_in(splits[13], 71), 0)
    keys = draw_keys(jax.random.fold_in(splits[13], 71), 0)
    values = normal_values(splits[2], (SEQUENCE_TOKENS, KV_HEADS * HD), 4.0, 20.0, ((0, 32),))
    gate_totals = draw_gate_totals(jax.random.fold_in(splits[13], 71), 0)
    documents = jnp.searchsorted(jnp.cumsum(ragged_sizes(splits[4], DOCS, SEQUENCE_TOKENS, DOC_MOST, 1)), jnp.arange(SEQUENCE_TOKENS), side="right").astype(jnp.int32)
    stream = normal_values(splits[5], (SEQUENCE_TOKENS, D), 0.5, 3.0, ((0, 32),))
    out_weight = normal_values(splits[6], (QUERY_HEAD_COUNT * HD, D), (QUERY_HEAD_COUNT * HD) ** -0.5, 0.1875)
    norm_gain = jnp.clip(1.0 + 0.18 * jax.random.normal(splits[7], (D,), jnp.float32), 0.1, 1.9)
    routes_keys = jax.random.split(jax.random.fold_in(splits[8], 1), SEQUENCE_TOKENS // (TOK_DEV // N_TP))
    routes_turns = jax.random.permutation(jax.random.fold_in(splits[8], 3), SEQUENCE_TOKENS // (TOK_DEV // N_TP))
    routes = jax.vmap(lambda own, number: assign_block(jax.random.fold_in(splits[8], 2), own, number, TOK_DEV // N_TP, EXPERTS, TOP, CAP, 1))(routes_keys, routes_turns).reshape((SEQUENCE_TOKENS, TOP))
    route_weights = jnp.clip(0.2 + 0.8 * jax.random.uniform(splits[9], (SEQUENCE_TOKENS, TOP), jnp.float32) ** shard_levels(splits[9], (SEQUENCE_TOKENS, TOP), ((0, 32),), -0.2, 0.2), 0.2, 1.0)
    expert_gate = normal_values(splits[10], (EXPERTS, D, FF), D ** -0.5, 0.125, ((0, 32),))
    expert_up = normal_values(splits[11], (EXPERTS, D, FF), D ** -0.5, 0.125, ((0, 32),))
    expert_down = normal_values(splits[12], (EXPERTS, FF, D), FF ** -0.5, 0.1875, ((0, 32),))
    return {"queries": queries, "keys": keys, "values": values, "gate_totals": gate_totals, "documents": documents, "stream": stream, "out_weight": out_weight, "norm_gain": norm_gain, "routes": routes, "route_weights": route_weights, "expert_gate": expert_gate, "expert_up": expert_up, "expert_down": expert_down}


EPS = 1e-06
MASKED = -1e+30

def attend(queries, keys, values, gate_totals, documents):
    group = QUERY_HEAD_COUNT // KV_HEADS
    block = min(256, SEQUENCE_TOKENS)
    scale = HD ** (-0.5)
    key_all = keys.astype(jnp.float32).reshape(SEQUENCE_TOKENS, KV_HEADS, HD)
    value_all = values.astype(jnp.float32).reshape(SEQUENCE_TOKENS, KV_HEADS, HD)
    key_gate = gate_totals.T.reshape(KV_HEADS, group, 1, SEQUENCE_TOKENS)
    key_pos = jnp.arange(SEQUENCE_TOKENS, dtype=jnp.int32)

    def one_block(index):
        start = (index * block).astype(jnp.int32)
        query_blk = lax.dynamic_slice_in_dim(queries, start, block, 0).astype(jnp.float32).reshape(block, KV_HEADS, group, HD)
        query_gate = lax.dynamic_slice_in_dim(gate_totals, start, block, 0).T.reshape(KV_HEADS, group, block, 1)
        query_doc = lax.dynamic_slice_in_dim(documents, start, block, 0)
        query_pos = start + jnp.arange(block, dtype=jnp.int32)
        scores = jnp.einsum('qkgd,skd->kgqs', query_blk, key_all) * scale + query_gate - key_gate
        allowed = (key_pos[None, :] <= query_pos[:, None]) & (documents[None, :] == query_doc[:, None])
        scores = jnp.where(allowed, scores, MASKED)
        highest = lax.optimization_barrier(jnp.max(scores, axis=-1, keepdims=True))
        weights = jnp.where(allowed, jnp.exp(scores - highest), 0.0)
        totals = lax.optimization_barrier(jnp.sum(weights, axis=-1))
        rounded = lax.optimization_barrier(weights.astype(jnp.bfloat16)).astype(jnp.float32)
        mixed = jnp.einsum('kgqs,skd->kgqd', rounded, value_all) / totals[..., None]
        return jnp.transpose(mixed, (2, 0, 1, 3)).reshape(block, QUERY_HEAD_COUNT * HD).astype(jnp.bfloat16)
    blocks = lax.map(one_block, jnp.arange(SEQUENCE_TOKENS // block, dtype=jnp.int32))
    return blocks.reshape(SEQUENCE_TOKENS, QUERY_HEAD_COUNT * HD)

def run_experts(normed, routes, expert_gate, expert_up, expert_down):
    flat = routes.reshape(-1)
    load = N_SP * N_TP * CAP
    half = FF // N_TP

    def one_expert(expert):
        rank_key = jnp.where(flat == expert, 0, 1).astype(jnp.int32)
        order = jnp.argsort(rank_key, stable=True)[:load].astype(jnp.int32)
        valid = flat[order] == expert
        picked = normed[order // TOP]
        gate = jnp.dot(picked, expert_gate[expert], preferred_element_type=jnp.float32)
        upper = jnp.dot(picked, expert_up[expert], preferred_element_type=jnp.float32)
        inner = (jax.nn.silu(gate) * upper).astype(jnp.bfloat16)
        answer = jnp.zeros((load, D), jnp.float32)
        for portion in range(N_TP):
            piece = jnp.dot(inner[:, portion * half:(portion + 1) * half], expert_down[expert][portion * half:(portion + 1) * half], preferred_element_type=jnp.float32)
            answer = answer + lax.optimization_barrier(piece.astype(jnp.bfloat16)).astype(jnp.float32)
        answer = jnp.where(valid[:, None], answer.astype(jnp.bfloat16).astype(jnp.float32), 0.0)
        return (order, answer)
    orders, answers = lax.map(one_expert, jnp.arange(EXPERTS, dtype=jnp.int32))
    entries = jnp.zeros((flat.shape[0], D), jnp.float32).at[orders.reshape(-1)].add(answers.reshape(-1, D))
    return entries.reshape(SEQUENCE_TOKENS, TOP, D)

def reference(queries, keys, values, gate_totals, documents, stream, out_weight, norm_gain, routes, route_weights, expert_gate, expert_up, expert_down):
    attended = attend(queries, keys, values, gate_totals, documents)
    hidden = (stream.astype(jnp.float32) + jnp.dot(attended, out_weight, preferred_element_type=jnp.float32)).astype(jnp.bfloat16)
    hidden_f = hidden.astype(jnp.float32)
    normed = (hidden_f * lax.rsqrt(lax.optimization_barrier(jnp.mean(hidden_f * hidden_f, axis=-1, keepdims=True)) + EPS) * norm_gain).astype(jnp.bfloat16)
    entries = run_experts(normed, routes, expert_gate, expert_up, expert_down)
    routed = lax.optimization_barrier(jnp.sum(route_weights[..., None] * entries, axis=1))
    return (hidden_f + routed).astype(jnp.bfloat16)
```

```python
import functools
import math

import jax
import jax.numpy as jnp
from jax import lax
from jax.experimental import pallas as pl
from jax.experimental.pallas import tpu as pltpu
from jax.sharding import PartitionSpec as P

QUERY_HEAD_COUNT = 16
KV_HEADS = 4
HD = 64
TOP = 2


EPS = 1e-06
MASKED = -1e30


def make_fold(query_rows, query_gate, key_gate_all, query_docs, first_pos, kv_local, group):
    count = query_rows.shape[0]
    scale = HD ** (-0.5)
    query_blk = query_rows.reshape(count, kv_local, group, HD)
    gate_here = query_gate.T.reshape(kv_local, group, count, 1)
    query_pos = first_pos + jnp.arange(count, dtype=jnp.int32)
    last_pos = first_pos + count - 1
    first_doc = query_docs[0]

    def block_step(carry, block_in):
        running_max, running_sum, carried = carry
        key_block, value_block, doc_block, pos_block = block_in
        width = key_block.shape[0]

        def compute(unused):
            key_heads = key_block.reshape(width, kv_local, HD)
            value_heads = value_block.reshape(width, kv_local, HD)
            gate_keys = lax.dynamic_slice_in_dim(key_gate_all, pos_block[0], width, 0).T.reshape(
                kv_local, group, 1, width
            )
            scores = (
                jnp.einsum(
                    "qkgd,nkd->kgqn", query_blk, key_heads, preferred_element_type=jnp.float32
                )
                * scale
                + gate_here
                - gate_keys
            )
            allowed = (pos_block[None, :] <= query_pos[:, None]) & (
                doc_block[None, :] == query_docs[:, None]
            )
            scores = jnp.where(allowed, scores, MASKED)
            new_max = jnp.maximum(running_max, jnp.max(scores, axis=-1))
            weights = jnp.where(allowed, jnp.exp(scores - new_max[..., None]), 0.0)
            factor = jnp.exp(running_max - new_max)
            new_sum = running_sum * factor + jnp.sum(weights, axis=-1)
            new_carried = carried * factor[..., None] + jnp.einsum(
                "kgqn,nkd->kgqd",
                weights.astype(jnp.bfloat16),
                value_heads,
                preferred_element_type=jnp.float32,
            )
            return (new_max, new_sum, new_carried)

        skipped = (pos_block[0] > last_pos) | (doc_block[width - 1] < first_doc)
        return (lax.cond(skipped, lambda unused: carry, compute, 0), None)

    def fold(carry, piece, start):
        key_piece, value_piece, doc_piece = piece
        length = key_piece.shape[0]
        width = math.gcd(length, 512)
        blocks_count = length // width
        pos_piece = jnp.arange(length, dtype=jnp.int32)
        blocks = (
            key_piece.reshape(blocks_count, width, -1),
            value_piece.reshape(blocks_count, width, -1),
            doc_piece.reshape(blocks_count, width),
            pos_piece.reshape(blocks_count, width),
        )
        carry, unused = lax.scan(block_step, carry, blocks)
        return carry

    initial = (
        jnp.full((kv_local, group, count), MASKED, jnp.float32),
        jnp.zeros((kv_local, group, count), jnp.float32),
        jnp.zeros((kv_local, group, count, HD), jnp.float32),
    )
    return (fold, initial)


def finish(running_sum, carried):
    mixed = carried / running_sum[..., None]
    count = mixed.shape[2]
    return jnp.transpose(mixed, (2, 0, 1, 3)).reshape(count, -1).astype(jnp.bfloat16)


def shards(
    queries,
    keys,
    values,
    gate_totals,
    documents,
    stream,
    out_weight,
    norm_gain,
    routes,
    route_weights,
    expert_gate,
    expert_up,
    expert_down,
):
    tp_count = lax.axis_size("tp")
    sp_count = lax.axis_size("sp")
    tp_index = lax.axis_index("tp")
    sp_index = lax.axis_index("sp")
    group = QUERY_HEAD_COUNT // KV_HEADS
    tok_local = queries.shape[0]
    own_rows = tok_local // tp_count
    first_row = sp_index * tok_local
    query_rows = lax.all_to_all(queries, "tp", split_axis=0, concat_axis=1, tiled=True)
    key_whole, value_whole = (
        lax.all_gather(keys, "tp", axis=1, tiled=True),
        lax.all_gather(values, "tp", axis=1, tiled=True),
    )
    gate_whole = lax.all_gather(gate_totals, "tp", axis=1, tiled=True)
    key_gate_all = lax.all_gather(gate_whole, "sp", axis=0, tiled=True)
    query_gate = lax.dynamic_slice_in_dim(gate_whole, tp_index * own_rows, own_rows, 0)
    query_docs = lax.dynamic_slice_in_dim(documents, tp_index * own_rows, own_rows, 0)
    fold, initial = make_fold(
        query_rows,
        query_gate,
        key_gate_all,
        query_docs,
        first_row + tp_index * own_rows,
        KV_HEADS,
        group,
    )
    running_max, running_sum, carried = fold(
        initial,
        (
            lax.all_gather(key_whole, "sp", axis=0, tiled=True),
            lax.all_gather(value_whole, "sp", axis=0, tiled=True),
            lax.all_gather(documents, "sp", axis=0, tiled=True),
        ),
        jnp.int32(0),
    )
    attended = finish(running_sum, carried)
    hidden = (
        stream.astype(jnp.float32)
        + jnp.dot(attended, out_weight, preferred_element_type=jnp.float32)
    ).astype(jnp.bfloat16)
    hidden_f = hidden.astype(jnp.float32)
    normed = (
        hidden_f
        * lax.rsqrt(jnp.mean(hidden_f * hidden_f, axis=-1, keepdims=True) + EPS)
        * norm_gain
    ).astype(jnp.bfloat16)
    local_experts = expert_gate.shape[0]
    experts_total = local_experts * sp_count
    capacity = max(2, 2 * tok_local * TOP // (tp_count * experts_total))
    flat = routes.reshape(-1)
    hits = (flat[:, None] == jnp.arange(experts_total, dtype=jnp.int32)[None, :]).astype(jnp.int32)
    slot_index = jnp.sum(jnp.cumsum(hits, axis=0) * hits, axis=1) - 1
    target = flat * capacity + slot_index
    entry_rows = jnp.repeat(normed, TOP, axis=0)
    outgoing = (
        jnp.zeros((experts_total * capacity, normed.shape[1]), jnp.bfloat16)
        .at[target]
        .set(entry_rows)
    )
    outgoing = outgoing.reshape(experts_total, capacity, -1)
    arrived = lax.all_to_all(outgoing, "sp", split_axis=0, concat_axis=0, tiled=True)
    slots = arrived.shape[1]
    both_halves = lax.all_gather(arrived, "tp", axis=0, tiled=True)
    grouped = both_halves.reshape(tp_count * sp_count, local_experts, slots, -1)
    gate = jnp.einsum("secd,edf->secf", grouped, expert_gate, preferred_element_type=jnp.float32)
    upper = jnp.einsum("secd,edf->secf", grouped, expert_up, preferred_element_type=jnp.float32)
    inner = (jax.nn.silu(gate) * upper).astype(jnp.bfloat16)
    partial_value = jnp.einsum(
        "secf,efd->secd", inner, expert_down, preferred_element_type=jnp.float32
    )
    partial_value = lax.optimization_barrier(partial_value.astype(jnp.bfloat16)).astype(jnp.float32)
    summed = lax.psum_scatter(
        partial_value.reshape(tp_count * sp_count * local_experts, slots, -1).astype(jnp.bfloat16),
        "tp",
        scatter_dimension=0,
        tiled=True,
    )
    returned = lax.all_to_all(summed, "sp", split_axis=0, concat_axis=0, tiled=True)
    answers = returned.reshape(experts_total * capacity, -1)[target].reshape(own_rows, TOP, -1)
    routed = jnp.sum(route_weights[..., None] * answers.astype(jnp.float32), axis=1)
    return (hidden_f + routed).astype(jnp.bfloat16)


def attend_kernel(sub, span, width, boundary_ref, query_ref, kv_ref, gate_ref, out_ref):
    tile = pl.program_id(0)
    stripes = kv_ref.shape[0]
    stripe = lax.rem(lax.axis_index("sp"), stripes)
    blocks = query_ref.shape[0]
    block = span // blocks
    group = QUERY_HEAD_COUNT // KV_HEADS
    rows = blocks * sub
    boundary = boundary_ref[0]
    first = tile * span
    per_tile = span // width
    taken = width // block
    zeros = jnp.zeros((rows, HD), jnp.bfloat16)
    query = query_ref[...].reshape(rows, group * HD) * jnp.bfloat16(HD ** (-0.5))
    stacked = jnp.concatenate(
        [
            jnp.concatenate([query[:, head * HD:(head + 1) * HD], zeros], axis=1)
            for head in range(group)
        ],
        axis=0,
    )
    row = lax.broadcasted_iota(jnp.int32, (rows, 1), 0)
    query_pos = first + (row // sub) * block + stripe * sub + lax.rem(row, sub)
    doc_start = jnp.where(query_pos >= boundary, boundary, 0)
    origin = gate_ref[tile * per_tile][:, :, 0:1]
    lane = lax.broadcasted_iota(jnp.int32, (width, 2 * HD), 1)

    def chunk(index, carry, masked):
        per_z = stripes // taken
        kv = kv_ref[pl.ds(lax.rem(index, per_z) * taken, taken), index // per_z, 0:block, :]
        kv = kv.reshape(width, 2 * HD)
        bias = origin - gate_ref[index]
        if masked:
            key_pos = index * width + lax.broadcasted_iota(jnp.int32, (1, width), 1)
            allowed = (key_pos <= query_pos) & (key_pos >= doc_start)
        scores = lax.dot_general(
            stacked, kv, (((1,), (1,)), ((), ())), preferred_element_type=jnp.float32
        )
        tops, mixed = carry
        new_tops, factors, weights = [], [], []
        for head in range(group):
            score = scores[head * rows:(head + 1) * rows] + bias[head]
            if masked:
                score = jnp.where(allowed, score, MASKED)
            new_top = jnp.maximum(tops[head], jnp.max(score, axis=1, keepdims=True))
            weight = jnp.exp(score - new_top)
            factor = jnp.exp(tops[head] - new_top)
            new_tops.append(new_top)
            factors.append(factor)
            weights.append(weight.astype(jnp.bfloat16))
        mixed = mixed * jnp.concatenate(factors, axis=0) + jnp.dot(
            jnp.concatenate(weights, axis=0),
            jnp.where(lane < HD, jnp.bfloat16(1), kv),
            preferred_element_type=jnp.float32,
        )
        return (tuple(new_tops), mixed)

    carry = (
        tuple(jnp.full((rows, 1), 0.5 * MASKED, jnp.float32) for unused in range(group)),
        jnp.zeros((group * rows, 2 * HD), jnp.float32),
    )
    own = tile * per_tile
    inside = (boundary > first) & (boundary < first + span)
    second = first >= boundary
    low = jnp.where(second, boundary // width, 0)
    clean_low = jnp.where(inside, own, jnp.where(second, (boundary + width - 1) // width, 0))
    clean_low = jnp.minimum(clean_low, own)
    carry = lax.fori_loop(low, clean_low, lambda i, c: chunk(i, c, True), carry)
    carry = lax.fori_loop(clean_low, own, lambda i, c: chunk(i, c, False), carry)
    carry = lax.fori_loop(own, own + per_tile, lambda i, c: chunk(i, c, True), carry)
    unused, mixed = carry
    ratio = mixed[:, HD:] / mixed[:, :HD]
    parts = [ratio[head * rows:(head + 1) * rows] for head in range(group)]
    out_ref[...] = jnp.concatenate(parts, axis=1).astype(jnp.bfloat16).reshape(out_ref.shape)


def exchange_kernel(
    stripes, kv_ref, query_ref, kv_all_ref, got_ref, z_send, z_recv, p_send, p_recv, s_send, s_recv, q_send, q_recv
):
    total = query_ref.shape[0]
    planes = total // stripes
    chips = stripes // 2
    me = lax.axis_index("sp")
    plane, spot = me // stripes, lax.rem(me, stripes)
    chip, core = spot // 2, lax.rem(spot, 2)
    partner = plane * stripes + chip * 2 + (1 - core)
    barrier = pltpu.get_barrier_semaphore()

    def greet(r, carry):
        pl.semaphore_signal(barrier, inc=1, device_id={"sp": lax.rem(me + r, total)})
        return carry

    lax.fori_loop(1, total, greet, 0)
    pl.semaphore_wait(barrier, total - 1)

    def along(r):
        other = lax.rem(plane + r, planes)
        return pltpu.make_async_remote_copy(
            src_ref=kv_ref.at[other],
            dst_ref=kv_all_ref.at[spot, plane],
            send_sem=z_send.at[r],
            recv_sem=z_recv.at[r],
            device_id={"sp": other * stripes + spot},
        )

    def block(r):
        if r == 0:
            return kv_ref.at[plane]
        return kv_all_ref.at[spot, lax.rem(plane + planes - r, planes)]

    def across(r, m):
        target = lax.rem(chip + m, chips)
        return pltpu.make_async_remote_copy(
            src_ref=block(r),
            dst_ref=kv_all_ref.at[spot, lax.rem(plane + planes - r, planes)],
            send_sem=p_send.at[r, m],
            recv_sem=p_recv.at[r, m],
            device_id={"sp": plane * stripes + target * 2 + core},
        )

    def over(r, m):
        source = lax.rem(chip + chips - m, chips) * 2 + core
        where = kv_all_ref.at[source, lax.rem(plane + planes - r, planes)]
        return pltpu.make_async_remote_copy(
            src_ref=block(r) if m == 0 else where,
            dst_ref=where,
            send_sem=s_send.at[r, m],
            recv_sem=s_recv.at[r, m],
            device_id={"sp": partner},
        )

    def direct(r):
        other = lax.rem(me + r, total)
        return pltpu.make_async_remote_copy(
            src_ref=query_ref.at[other],
            dst_ref=got_ref.at[me],
            send_sem=q_send.at[r],
            recv_sem=q_recv.at[r],
            device_id={"sp": other},
        )

    order = sorted(range(1, planes), key=lambda r: min(r, planes - r))
    for r in order:
        along(r).start()
    for m in range(1, chips):
        across(0, m).start()
    over(0, 0).start()

    def send_query(r, carry):
        direct(r).start()
        return carry

    lax.fori_loop(1, total, send_query, 0)
    kv_all_ref[spot, plane] = kv_ref[plane]
    got_ref[me] = query_ref[me]
    for at, r in enumerate(order):
        along(r).wait_recv()
        for m in range(1, chips):
            across(r, m).start()
        over(r, 0).start()
        earlier = 0 if at == 0 else order[at - 1]
        for m in range(1, chips):
            across(earlier, m).wait_recv()
            over(earlier, m).start()
    for m in range(1, chips):
        across(order[-1], m).wait_recv()
        over(order[-1], m).start()
    for r in range(planes):
        for m in range(chips):
            over(r, m).wait()
    for r in range(1, planes):
        along(r).wait_send()
    for r in range(planes):
        for m in range(1, chips):
            across(r, m).wait_send()

    def end_query(r, carry):
        direct(r).wait()
        return carry

    lax.fori_loop(1, total, end_query, 0)


def exchange(message, query_send, stripes):
    total = query_send.shape[0]
    planes, chips = total // stripes, stripes // 2
    vmem = pl.BlockSpec(memory_space=pltpu.VMEM)
    dma = pltpu.SemaphoreType.DMA
    return pl.pallas_call(
        functools.partial(exchange_kernel, stripes),
        in_specs=[vmem, vmem],
        out_specs=[vmem, vmem],
        out_shape=[
            jax.ShapeDtypeStruct((stripes,) + message.shape, message.dtype),
            jax.ShapeDtypeStruct(query_send.shape, query_send.dtype),
        ],
        scratch_shapes=[
            dma((planes,)),
            dma((planes,)),
            dma((planes, chips)),
            dma((planes, chips)),
            dma((planes, chips)),
            dma((planes, chips)),
            dma((total,)),
            dma((total,)),
        ],
        compiler_params=pltpu.CompilerParams(
            collective_id=0, has_side_effects=True, vmem_limit_bytes=24 * 1024 * 1024
        ),
        name="exchange",
    )(message, query_send)


def fast_shards(
    queries,
    keys,
    values,
    gate_totals,
    documents,
    stream,
    out_weight,
    norm_gain,
    routes,
    route_weights,
    expert_gate,
    expert_up,
    expert_down,
):
    sp_count = lax.axis_size("sp")
    group = QUERY_HEAD_COUNT // KV_HEADS
    tok = queries.shape[0]
    stripes = sp_count // KV_HEADS
    sub = tok // stripes
    blocks = 4
    span = blocks * tok
    width = min(span, 1024)
    tiles = sp_count // blocks
    lanes = 2 * HD
    part_a = lax.reduce_precision(gate_totals, 8, 7)
    rest = gate_totals - part_a
    part_b = lax.reduce_precision(rest, 8, 7)
    part_c = rest - part_b
    parts = jnp.stack([part_a, part_b, part_c], axis=0).astype(jnp.bfloat16)
    parts = jnp.transpose(parts.reshape(3, tok, KV_HEADS, group), (2, 0, 3, 1))
    parts = parts.reshape(KV_HEADS, 3 * group, tok)
    docs = jnp.broadcast_to(documents.astype(jnp.bfloat16)[None, None, :], (KV_HEADS, 4, tok))
    extra = jnp.concatenate([parts, docs], axis=1).reshape(KV_HEADS, -1, lanes)
    kv = jnp.concatenate(
        [keys.reshape(tok, KV_HEADS, HD), values.reshape(tok, KV_HEADS, HD)], axis=2
    )
    message = jnp.concatenate([jnp.transpose(kv, (1, 0, 2)), extra], axis=1)
    query_send = jnp.transpose(
        queries.reshape(stripes, sub, KV_HEADS, group * HD), (2, 0, 1, 3)
    ).reshape(sp_count, sub, group * HD)
    kv_all, query_got = exchange(message, query_send, stripes)
    extra_all = jnp.transpose(kv_all[:, :, tok:, :], (1, 0, 2, 3)).reshape(sp_count, 16, tok)
    extra_all = extra_all.astype(jnp.float32)
    boundary = jnp.sum((extra_all[:, 3 * group, :] < 0.5).astype(jnp.int32)).reshape(1)
    gates = extra_all[:, :group] + extra_all[:, group:2 * group] + extra_all[:, 2 * group:3 * group]
    gates = jnp.transpose(gates.reshape(tiles, blocks, group, tok), (0, 2, 1, 3))
    gates = jnp.transpose(gates.reshape(tiles, group, span // width, 1, width), (0, 2, 1, 3, 4))
    gates = gates.reshape(-1, group, 1, width)
    mixed = pl.pallas_call(
        functools.partial(attend_kernel, sub, span, width),
        grid=(tiles,),
        in_specs=[
            pl.BlockSpec(memory_space=pltpu.SMEM),
            pl.BlockSpec((blocks, sub, group * HD), lambda i: (i, 0, 0)),
            pl.BlockSpec(kv_all.shape, lambda i: (0, 0, 0, 0)),
            pl.BlockSpec(gates.shape, lambda i: (0, 0, 0, 0)),
        ],
        out_specs=pl.BlockSpec((blocks, sub, group * HD), lambda i: (i, 0, 0)),
        out_shape=jax.ShapeDtypeStruct((sp_count, sub, group * HD), jnp.bfloat16),
        compiler_params=pltpu.CompilerParams(vmem_limit_bytes=48 * 1024 * 1024),
        name="attend",
    )(boundary, query_got, kv_all, gates)
    back = lax.all_to_all(mixed, "sp", split_axis=0, concat_axis=0, tiled=True)
    attended = jnp.transpose(
        back.reshape(KV_HEADS, stripes, sub, group * HD), (1, 2, 0, 3)
    ).reshape(tok, QUERY_HEAD_COUNT * HD)
    hidden = (
        stream.astype(jnp.float32)
        + jnp.dot(attended, out_weight, preferred_element_type=jnp.float32)
    ).astype(jnp.bfloat16)
    hidden_f = hidden.astype(jnp.float32)
    normed = (
        hidden_f
        * lax.rsqrt(jnp.mean(hidden_f * hidden_f, axis=-1, keepdims=True) + EPS)
        * norm_gain
    ).astype(jnp.bfloat16)
    experts_total = sp_count
    capacity = max(2, 2 * tok * TOP // experts_total)
    slots = experts_total * capacity
    flat = routes.reshape(-1)
    hits = (flat[:, None] == jnp.arange(experts_total, dtype=jnp.int32)[None, :]).astype(jnp.int32)
    slot_index = jnp.sum(jnp.cumsum(hits, axis=0) * hits, axis=1) - 1
    target = (flat * capacity + slot_index).reshape(tok, TOP)
    line = jnp.arange(slots, dtype=jnp.int32)
    placed = sum(
        (line[:, None] == target[:, k][None, :]).astype(jnp.bfloat16) for k in range(TOP)
    )
    outgoing = jnp.dot(placed, normed, preferred_element_type=jnp.float32).astype(jnp.bfloat16)
    arrived = lax.all_to_all(
        outgoing.reshape(experts_total, capacity, -1), "sp", split_axis=0, concat_axis=0, tiled=True
    ).reshape(slots, -1)
    gate = jnp.dot(arrived, expert_gate[0], preferred_element_type=jnp.float32)
    upper = jnp.dot(arrived, expert_up[0], preferred_element_type=jnp.float32)
    inner = (jax.nn.silu(gate) * upper).astype(jnp.bfloat16)
    answer = jnp.dot(inner, expert_down[0], preferred_element_type=jnp.float32).astype(jnp.bfloat16)
    returned = lax.all_to_all(
        answer.reshape(sp_count, capacity, -1), "sp", split_axis=0, concat_axis=0, tiled=True
    ).reshape(slots, -1)
    share = sum(
        jnp.where(line[None, :] == target[:, k][:, None], route_weights[:, k][:, None], 0.0)
        for k in range(TOP)
    )
    share_high = lax.reduce_precision(share, 8, 7)
    share_low = (share - share_high).astype(jnp.bfloat16)
    routed = jnp.dot(
        share_high.astype(jnp.bfloat16), returned, preferred_element_type=jnp.float32
    ) + jnp.dot(share_low, returned, preferred_element_type=jnp.float32)
    return (hidden_f + routed).astype(jnp.bfloat16)


def solution(mesh):
    sp_count, tp_count = mesh.shape["sp"], mesh.shape["tp"]
    fast = tp_count == 1 and sp_count % (2 * KV_HEADS) == 0
    return jax.shard_map(
        fast_shards if fast else shards,
        mesh=mesh,
        in_specs=(
            P("sp", "tp"),
            P("sp", "tp"),
            P("sp", "tp"),
            P("sp", "tp"),
            P("sp"),
            P(("sp", "tp"), None),
            P(),
            P(),
            P(("sp", "tp"), None),
            P(("sp", "tp"), None),
            P("sp", None, "tp"),
            P("sp", None, "tp"),
            P("sp", "tp", None),
        ),
        out_specs=P(("sp", "tp"), None),
        check_vma=False,
    )
```

```python
import functools
import math

import jax
import jax.numpy as jnp
from jax import lax
from jax.experimental import pallas as pl
from jax.experimental.pallas import tpu as pltpu
from jax.sharding import PartitionSpec as P

QUERY_HEAD_COUNT = 16
KV_HEADS = 4
HD = 64
TOP = 2


EPS = 1e-06
MASKED = -1e30


def make_fold(query_rows, query_gate, key_gate_all, query_docs, first_pos, kv_local, group):
    count = query_rows.shape[0]
    scale = HD ** (-0.5)
    query_blk = query_rows.reshape(count, kv_local, group, HD)
    gate_here = query_gate.T.reshape(kv_local, group, count, 1)
    query_pos = first_pos + jnp.arange(count, dtype=jnp.int32)
    last_pos = first_pos + count - 1
    first_doc = query_docs[0]

    def block_step(carry, block_in):
        running_max, running_sum, carried = carry
        key_block, value_block, doc_block, pos_block = block_in
        width = key_block.shape[0]

        def compute(unused):
            key_heads = key_block.reshape(width, kv_local, HD)
            value_heads = value_block.reshape(width, kv_local, HD)
            gate_keys = lax.dynamic_slice_in_dim(key_gate_all, pos_block[0], width, 0).T.reshape(
                kv_local, group, 1, width
            )
            scores = (
                jnp.einsum(
                    "qkgd,nkd->kgqn", query_blk, key_heads, preferred_element_type=jnp.float32
                )
                * scale
                + gate_here
                - gate_keys
            )
            allowed = (pos_block[None, :] <= query_pos[:, None]) & (
                doc_block[None, :] == query_docs[:, None]
            )
            scores = jnp.where(allowed, scores, MASKED)
            new_max = jnp.maximum(running_max, jnp.max(scores, axis=-1))
            weights = jnp.where(allowed, jnp.exp(scores - new_max[..., None]), 0.0)
            factor = jnp.exp(running_max - new_max)
            new_sum = running_sum * factor + jnp.sum(weights, axis=-1)
            new_carried = carried * factor[..., None] + jnp.einsum(
                "kgqn,nkd->kgqd",
                weights.astype(jnp.bfloat16),
                value_heads,
                preferred_element_type=jnp.float32,
            )
            return (new_max, new_sum, new_carried)

        skipped = (pos_block[0] > last_pos) | (doc_block[width - 1] < first_doc)
        return (lax.cond(skipped, lambda unused: carry, compute, 0), None)

    def fold(carry, piece, start):
        key_piece, value_piece, doc_piece = piece
        length = key_piece.shape[0]
        width = math.gcd(length, 512)
        blocks_count = length // width
        pos_piece = jnp.arange(length, dtype=jnp.int32)
        blocks = (
            key_piece.reshape(blocks_count, width, -1),
            value_piece.reshape(blocks_count, width, -1),
            doc_piece.reshape(blocks_count, width),
            pos_piece.reshape(blocks_count, width),
        )
        carry, unused = lax.scan(block_step, carry, blocks)
        return carry

    initial = (
        jnp.full((kv_local, group, count), MASKED, jnp.float32),
        jnp.zeros((kv_local, group, count), jnp.float32),
        jnp.zeros((kv_local, group, count, HD), jnp.float32),
    )
    return (fold, initial)


def finish(running_sum, carried):
    mixed = carried / running_sum[..., None]
    count = mixed.shape[2]
    return jnp.transpose(mixed, (2, 0, 1, 3)).reshape(count, -1).astype(jnp.bfloat16)


def shards(
    queries,
    keys,
    values,
    gate_totals,
    documents,
    stream,
    out_weight,
    norm_gain,
    routes,
    route_weights,
    expert_gate,
    expert_up,
    expert_down,
):
    tp_count = lax.axis_size("tp")
    sp_count = lax.axis_size("sp")
    tp_index = lax.axis_index("tp")
    sp_index = lax.axis_index("sp")
    group = QUERY_HEAD_COUNT // KV_HEADS
    tok_local = queries.shape[0]
    own_rows = tok_local // tp_count
    first_row = sp_index * tok_local
    query_rows = lax.all_to_all(queries, "tp", split_axis=0, concat_axis=1, tiled=True)
    key_whole, value_whole = (
        lax.all_gather(keys, "tp", axis=1, tiled=True),
        lax.all_gather(values, "tp", axis=1, tiled=True),
    )
    gate_whole = lax.all_gather(gate_totals, "tp", axis=1, tiled=True)
    key_gate_all = lax.all_gather(gate_whole, "sp", axis=0, tiled=True)
    query_gate = lax.dynamic_slice_in_dim(gate_whole, tp_index * own_rows, own_rows, 0)
    query_docs = lax.dynamic_slice_in_dim(documents, tp_index * own_rows, own_rows, 0)
    fold, initial = make_fold(
        query_rows,
        query_gate,
        key_gate_all,
        query_docs,
        first_row + tp_index * own_rows,
        KV_HEADS,
        group,
    )
    running_max, running_sum, carried = fold(
        initial,
        (
            lax.all_gather(key_whole, "sp", axis=0, tiled=True),
            lax.all_gather(value_whole, "sp", axis=0, tiled=True),
            lax.all_gather(documents, "sp", axis=0, tiled=True),
        ),
        jnp.int32(0),
    )
    attended = finish(running_sum, carried)
    hidden = (
        stream.astype(jnp.float32)
        + jnp.dot(attended, out_weight, preferred_element_type=jnp.float32)
    ).astype(jnp.bfloat16)
    hidden_f = hidden.astype(jnp.float32)
    normed = (
        hidden_f
        * lax.rsqrt(jnp.mean(hidden_f * hidden_f, axis=-1, keepdims=True) + EPS)
        * norm_gain
    ).astype(jnp.bfloat16)
    local_experts = expert_gate.shape[0]
    experts_total = local_experts * sp_count
    capacity = max(2, 2 * tok_local * TOP // (tp_count * experts_total))
    flat = routes.reshape(-1)
    hits = (flat[:, None] == jnp.arange(experts_total, dtype=jnp.int32)[None, :]).astype(jnp.int32)
    slot_index = jnp.sum(jnp.cumsum(hits, axis=0) * hits, axis=1) - 1
    target = flat * capacity + slot_index
    entry_rows = jnp.repeat(normed, TOP, axis=0)
    outgoing = (
        jnp.zeros((experts_total * capacity, normed.shape[1]), jnp.bfloat16)
        .at[target]
        .set(entry_rows)
    )
    outgoing = outgoing.reshape(experts_total, capacity, -1)
    arrived = lax.all_to_all(outgoing, "sp", split_axis=0, concat_axis=0, tiled=True)
    slots = arrived.shape[1]
    both_halves = lax.all_gather(arrived, "tp", axis=0, tiled=True)
    grouped = both_halves.reshape(tp_count * sp_count, local_experts, slots, -1)
    gate = jnp.einsum("secd,edf->secf", grouped, expert_gate, preferred_element_type=jnp.float32)
    upper = jnp.einsum("secd,edf->secf", grouped, expert_up, preferred_element_type=jnp.float32)
    inner = (jax.nn.silu(gate) * upper).astype(jnp.bfloat16)
    partial_value = jnp.einsum(
        "secf,efd->secd", inner, expert_down, preferred_element_type=jnp.float32
    )
    partial_value = lax.optimization_barrier(partial_value.astype(jnp.bfloat16)).astype(jnp.float32)
    summed = lax.psum_scatter(
        partial_value.reshape(tp_count * sp_count * local_experts, slots, -1).astype(jnp.bfloat16),
        "tp",
        scatter_dimension=0,
        tiled=True,
    )
    returned = lax.all_to_all(summed, "sp", split_axis=0, concat_axis=0, tiled=True)
    answers = returned.reshape(experts_total * capacity, -1)[target].reshape(own_rows, TOP, -1)
    routed = jnp.sum(route_weights[..., None] * answers.astype(jnp.float32), axis=1)
    return (hidden_f + routed).astype(jnp.bfloat16)


def attend_kernel(sub, span, width, query_ref, kv_ref, notes_ref, out_ref, boundary_ref):
    tile = pl.program_id(0)
    stripes = kv_ref.shape[0]
    stripe = lax.rem(lax.axis_index("sp"), stripes)
    blocks = query_ref.shape[0]
    block = span // blocks
    group = QUERY_HEAD_COUNT // KV_HEADS
    rows = blocks * sub

    @pl.when(tile == 0)
    def count():
        earlier = notes_ref[:, :, group:group + 1, :] < 0.5
        boundary_ref[0] = jnp.sum(earlier.astype(jnp.float32)).astype(jnp.int32)

    boundary = boundary_ref[0]
    first = tile * span
    per_tile = span // width
    taken = width // block
    zeros = jnp.zeros((rows, HD), jnp.bfloat16)
    query = query_ref[...].reshape(rows, group * HD) * jnp.bfloat16(HD ** (-0.5))
    stacked = jnp.concatenate(
        [
            jnp.concatenate([query[:, head * HD:(head + 1) * HD], zeros], axis=1)
            for head in range(group)
        ],
        axis=0,
    )
    row = lax.broadcasted_iota(jnp.int32, (rows, 1), 0)
    query_pos = first + (row // sub) * block + stripe * sub + lax.rem(row, sub)
    doc_start = jnp.where(query_pos >= boundary, boundary, 0)
    per_z = stripes // taken

    def gate_rows(index):
        block_notes = notes_ref[pl.ds(lax.rem(index, per_z) * taken, taken), index // per_z]
        return [
            jnp.concatenate(
                [block_notes[at, head:head + 1, :] for at in range(taken)], axis=1
            )
            for head in range(group)
        ]

    origin = [gate[:, 0:1] for gate in gate_rows(tile * per_tile)]
    lane = lax.broadcasted_iota(jnp.int32, (width, 2 * HD), 1)

    def chunk(index, carry, masked):
        kv = kv_ref[pl.ds(lax.rem(index, per_z) * taken, taken), index // per_z]
        kv = kv.reshape(width, 2 * HD)
        bias = [start - gate for start, gate in zip(origin, gate_rows(index))]
        if masked:
            key_pos = index * width + lax.broadcasted_iota(jnp.int32, (1, width), 1)
            allowed = (key_pos <= query_pos) & (key_pos >= doc_start)
        scores = lax.dot_general(
            stacked, kv, (((1,), (1,)), ((), ())), preferred_element_type=jnp.float32
        )
        tops, mixed = carry
        new_tops, factors, weights = [], [], []
        for head in range(group):
            score = scores[head * rows:(head + 1) * rows] + bias[head]
            if masked:
                score = jnp.where(allowed, score, MASKED)
            new_top = jnp.maximum(tops[head], jnp.max(score, axis=1, keepdims=True))
            weight = jnp.exp(score - new_top)
            factor = jnp.exp(tops[head] - new_top)
            new_tops.append(new_top)
            factors.append(factor)
            weights.append(weight.astype(jnp.bfloat16))
        mixed = mixed * jnp.concatenate(factors, axis=0) + jnp.dot(
            jnp.concatenate(weights, axis=0),
            jnp.where(lane < HD, jnp.bfloat16(1), kv),
            preferred_element_type=jnp.float32,
        )
        return (tuple(new_tops), mixed)

    carry = (
        tuple(jnp.full((rows, 1), 0.5 * MASKED, jnp.float32) for unused in range(group)),
        jnp.zeros((group * rows, 2 * HD), jnp.float32),
    )
    own = tile * per_tile
    inside = (boundary > first) & (boundary < first + span)
    second = first >= boundary
    low = jnp.where(second, boundary // width, 0)
    clean_low = jnp.where(inside, own, jnp.where(second, (boundary + width - 1) // width, 0))
    clean_low = jnp.minimum(clean_low, own)
    carry = lax.fori_loop(low, clean_low, lambda i, c: chunk(i, c, True), carry)
    carry = lax.fori_loop(clean_low, own, lambda i, c: chunk(i, c, False), carry)
    carry = lax.fori_loop(own, own + per_tile, lambda i, c: chunk(i, c, True), carry)
    unused, mixed = carry
    ratio = mixed[:, HD:] / mixed[:, :HD]
    parts = [ratio[head * rows:(head + 1) * rows] for head in range(group)]
    out_ref[...] = jnp.concatenate(parts, axis=1).astype(jnp.bfloat16).reshape(out_ref.shape)


def exchange_kernel(
    stripes,
    keys_ref,
    values_ref,
    query_ref,
    notes_ref,
    kv_all_ref,
    got_ref,
    notes_all_ref,
    kv_ref,
    z_send,
    z_recv,
    p_send,
    p_recv,
    s_send,
    s_recv,
    q_send,
    q_recv,
):
    total, sub, wide = got_ref.shape
    planes = total // stripes
    chips = stripes // 2
    me = lax.axis_index("sp")
    plane, spot = me // stripes, lax.rem(me, stripes)
    chip, core = spot // 2, lax.rem(spot, 2)
    partner = plane * stripes + chip * 2 + (1 - core)
    barrier = pltpu.get_barrier_semaphore()

    def greet(r, carry):
        pl.semaphore_signal(barrier, inc=1, device_id={"sp": lax.rem(me + r, total)})
        return carry

    lax.fori_loop(1, total, greet, 0)
    for g in range(planes):
        part = slice(g * HD, (g + 1) * HD)
        kv_ref[g] = jnp.concatenate([keys_ref[:, part], values_ref[:, part]], axis=1)
    pl.semaphore_wait(barrier, total - 1)
    sources, targets = (kv_ref, notes_ref), (kv_all_ref, notes_all_ref)

    def along(r, n):
        other = lax.rem(plane + r, planes)
        return pltpu.make_async_remote_copy(
            src_ref=sources[n].at[other],
            dst_ref=targets[n].at[spot, plane],
            send_sem=z_send.at[n, r],
            recv_sem=z_recv.at[n, r],
            device_id={"sp": other * stripes + spot},
        )

    def origin(r):
        return lax.rem(plane + planes - r, planes)

    def block(r, n):
        if r == 0:
            return sources[n].at[plane]
        return targets[n].at[spot, origin(r)]

    def across(r, m, n):
        target = lax.rem(chip + m, chips)
        return pltpu.make_async_remote_copy(
            src_ref=block(r, n),
            dst_ref=targets[n].at[spot, origin(r)],
            send_sem=p_send.at[n, r, m],
            recv_sem=p_recv.at[n, r, m],
            device_id={"sp": plane * stripes + target * 2 + core},
        )

    def over(r, m, n):
        source = lax.rem(chip + chips - m, chips) * 2 + core
        where = targets[n].at[source, origin(r)]
        return pltpu.make_async_remote_copy(
            src_ref=block(r, n) if m == 0 else where,
            dst_ref=where,
            send_sem=s_send.at[n, r, m],
            recv_sem=s_recv.at[n, r, m],
            device_id={"sp": partner},
        )

    def piece(other):
        head, stripe = other // stripes, lax.rem(other, stripes)
        return (
            pl.ds(pl.multiple_of(stripe * sub, sub), sub),
            pl.ds(pl.multiple_of(head * wide, wide), wide),
        )

    def direct(r):
        other = lax.rem(me + r, total)
        return pltpu.make_async_remote_copy(
            src_ref=query_ref.at[piece(other)],
            dst_ref=got_ref.at[me],
            send_sem=q_send.at[r],
            recv_sem=q_recv.at[r],
            device_id={"sp": other},
        )

    both = (0, 1)
    order = sorted(range(1, planes), key=lambda r: min(r, planes - r))
    for r in order:
        for n in both:
            along(r, n).start()
    for m in range(1, chips):
        for n in both:
            across(0, m, n).start()
    for n in both:
        over(0, 0, n).start()

    def send_query(r, carry):
        direct(r).start()
        return carry

    lax.fori_loop(1, total, send_query, 0)
    kv_all_ref[spot, plane] = kv_ref[plane]
    notes_all_ref[spot, plane] = notes_ref[plane]
    got_ref[me] = query_ref[piece(me)]
    for at, r in enumerate(order):
        for n in both:
            along(r, n).wait_recv()
            for m in range(1, chips):
                across(r, m, n).start()
            over(r, 0, n).start()
        earlier = 0 if at == 0 else order[at - 1]
        for m in range(1, chips):
            for n in both:
                across(earlier, m, n).wait_recv()
                over(earlier, m, n).start()
    for m in range(1, chips):
        for n in both:
            across(order[-1], m, n).wait_recv()
            over(order[-1], m, n).start()
    for n in both:
        for r in range(planes):
            for m in range(chips):
                over(r, m, n).wait()
        for r in range(1, planes):
            along(r, n).wait_send()
        for r in range(planes):
            for m in range(1, chips):
                across(r, m, n).wait_send()

    def end_query(r, carry):
        direct(r).wait()
        return carry

    lax.fori_loop(1, total, end_query, 0)


def exchange(keys, values, queries, notes, stripes):
    planes, chips = notes.shape[0], stripes // 2
    total, tok = planes * stripes, keys.shape[0]
    got = (total, tok // stripes, queries.shape[1] // planes)
    vmem = pl.BlockSpec(memory_space=pltpu.VMEM)
    dma = pltpu.SemaphoreType.DMA
    return pl.pallas_call(
        functools.partial(exchange_kernel, stripes),
        in_specs=[vmem] * 4,
        out_specs=[vmem] * 3,
        out_shape=[
            jax.ShapeDtypeStruct((stripes, planes, tok, 2 * HD), keys.dtype),
            jax.ShapeDtypeStruct(got, queries.dtype),
            jax.ShapeDtypeStruct((stripes,) + notes.shape, notes.dtype),
        ],
        scratch_shapes=[
            pltpu.VMEM((planes, tok, 2 * HD), keys.dtype),
            dma((2, planes)),
            dma((2, planes)),
            dma((2, planes, chips)),
            dma((2, planes, chips)),
            dma((2, planes, chips)),
            dma((2, planes, chips)),
            dma((total,)),
            dma((total,)),
        ],
        compiler_params=pltpu.CompilerParams(
            collective_id=0, has_side_effects=True, vmem_limit_bytes=24 * 1024 * 1024
        ),
        name="exchange",
    )(keys, values, queries, notes)


def mixture_kernel(
    capacity,
    stripes,
    slots,
    mixed_ref,
    stream_ref,
    gain_ref,
    rows_ref,
    columns_ref,
    weights_ref,
    begin_row_ref,
    begin_ref,
    project_hbm,
    gate_hbm,
    up_hbm,
    down_hbm,
    out_ref,
    project_w,
    gate_w,
    up_w,
    down_w,
    attended,
    hidden_ref,
    normed_ref,
    packed,
    landed,
    sending,
    arrived,
    inner,
    answers,
    returned,
    got,
    total,
    w_sem,
    h_send,
    h_recv,
    z_send,
    z_recv,
    a_send,
    a_recv,
    b_send,
    b_recv,
    r_send,
    r_recv,
):
    planes = begin_ref.shape[0]
    devices = planes * stripes
    tok, width = stream_ref.shape
    sub, wide = mixed_ref.shape[1:]
    backing = landed
    hidden_units = gate_w.shape[1]
    rows = stripes * slots
    step = math.gcd(width, 256)
    me = lax.axis_index("sp")
    plane, spot = me // stripes, lax.rem(me, stripes)

    def plane_of(m):
        if m == 1:
            return plane + 1 - 2 * lax.rem(plane, 2)
        if m == 2:
            return lax.rem(plane + 2, 4)
        return plane if m == 0 else 3 - plane

    barrier = pltpu.get_barrier_semaphore()

    def greet(r, carry):
        pl.semaphore_signal(barrier, inc=1, device_id={"sp": lax.rem(me + r, devices)})
        return carry

    lax.fori_loop(1, devices, greet, 0)
    weights = [
        pltpu.make_async_copy(source, target, w_sem.at[at])
        for at, (source, target) in enumerate(
            (
                (project_hbm, project_w),
                (gate_hbm.at[0], gate_w),
                (up_hbm.at[0], up_w),
                (down_hbm.at[0], down_w),
            )
        )
    ]
    for copy in weights:
        copy.start()
    pl.semaphore_wait(barrier, devices - 1)

    def home(owner):
        head, stripe = owner // stripes, lax.rem(owner, stripes)
        return (
            pl.ds(pl.multiple_of(stripe * sub, sub), sub),
            pl.ds(pl.multiple_of(head * wide, wide), wide),
        )

    def home_copy(r):
        other = lax.rem(me + r, devices)
        return pltpu.make_async_remote_copy(
            src_ref=mixed_ref.at[other],
            dst_ref=attended.at[home(me)],
            send_sem=h_send.at[r],
            recv_sem=h_recv.at[r],
            device_id={"sp": other},
        )

    def send_home(r, carry):
        home_copy(r).start()
        return carry

    def wait_home(r, carry):
        home_copy(r).wait()
        return carry

    lax.fori_loop(1, devices, send_home, 0)
    attended[home(me)] = mixed_ref[me]
    lax.fori_loop(1, devices, wait_home, 0)
    weights[0].wait()

    def project(index, squares):
        cols = pl.ds(pl.multiple_of(index * step, step), step)
        product = jnp.dot(attended[...], project_w[:, cols], preferred_element_type=jnp.float32)
        hidden = (stream_ref[:, cols].astype(jnp.float32) + product).astype(jnp.bfloat16)
        hidden_ref[:, cols] = hidden
        wider = hidden.astype(jnp.float32)
        return squares + jnp.sum(wider * wider, axis=1, keepdims=True)

    squares = lax.fori_loop(0, width // step, project, jnp.zeros((tok, 1), jnp.float32))
    inverse = lax.rsqrt(squares / width + EPS)

    def columns(body, length, size):
        def at(index, carry):
            body(pl.ds(pl.multiple_of(index * size, size), size))
            return carry

        lax.fori_loop(0, length // size, at, 0)

    def dot(left, right):
        return jnp.dot(left, right, preferred_element_type=jnp.float32)

    def norm(cols):
        scaled = hidden_ref[:, cols].astype(jnp.float32) * inverse * gain_ref[:, cols]
        normed_ref[:, cols] = scaled.astype(jnp.bfloat16)

    columns(norm, width, step)
    high_slot = lax.broadcasted_iota(jnp.int32, (capacity, 1), 0)
    low_slot = lax.broadcasted_iota(jnp.int32, (1, capacity), 1)

    def chosen_of(hit):
        return jnp.where(hit, 1.0, 0.0)

    def out_copy(m):
        return pltpu.make_async_remote_copy(
            src_ref=packed.at[m],
            dst_ref=landed.at[m],
            send_sem=z_send.at[m],
            recv_sem=z_recv.at[m],
            device_id={"sp": plane_of(m) * stripes + spot},
        )

    def back_copy(m):
        return pltpu.make_async_remote_copy(
            src_ref=backing.at[m],
            dst_ref=got.at[m],
            send_sem=r_send.at[m],
            recv_sem=r_recv.at[m],
            device_id={"sp": plane_of(m) * stripes + spot},
        )

    def near_copy(source, target, send, recv, m, i):
        other = lax.rem(spot + i, stripes)
        return pltpu.make_async_remote_copy(
            src_ref=source.at[m, other],
            dst_ref=target.at[m, spot],
            send_sem=send.at[m, i],
            recv_sem=recv.at[m, i],
            device_id={"sp": plane * stripes + other},
        )

    def to_expert(m, i):
        return near_copy(sending, arrived, a_send, a_recv, m, i)

    def from_expert(m, i):
        return near_copy(answers, returned, b_send, b_recv, m, i)

    def pack(m):
        begins = plane_of(m) * rows
        hits = sum(chosen_of(rows_ref[k:k + 1] - begins == high_slot) for k in range(TOP))
        hits = hits.astype(jnp.bfloat16)

        def body(cols):
            packed[m, :, cols] = dot(hits, normed_ref[:, cols]).astype(jnp.bfloat16)

        columns(body, width, step)

    def spread(m):
        hits = chosen_of(begin_ref[plane_of(m)] == low_slot).astype(jnp.bfloat16)
        source = packed if m == 0 else landed
        if m:
            out_copy(m).wait_recv()

        def body(cols):
            chosen = dot(hits, source[m, :, cols]).astype(jnp.bfloat16)
            sending[m, :, :, cols] = chosen.reshape(stripes, slots, step)

        columns(body, width, step)
        arrived[m, spot] = sending[m, spot]
        for i in range(1, stripes):
            to_expert(m, i).start()

    def compute(m):
        for i in range(1, stripes):
            to_expert(m, i).wait_recv()

        def middle(cols):
            rows_in = arrived[m].reshape(rows, width)
            gate = dot(rows_in, gate_w[:, cols])
            upper = dot(rows_in, up_w[:, cols])
            inner[:, cols] = (jax.nn.silu(gate) * upper).astype(jnp.bfloat16)

        columns(middle, hidden_units, math.gcd(hidden_units, 256))

        def last(cols):
            answer = dot(inner[...], down_w[:, cols]).astype(jnp.bfloat16)
            answers[m, :, :, cols] = answer.reshape(stripes, slots, step)

        columns(last, width, step)
        returned[m, spot] = answers[m, spot]
        for i in range(1, stripes):
            from_expert(m, i).start()

    def collect(m):
        hits = chosen_of(begin_row_ref[plane_of(m)] == high_slot).astype(jnp.bfloat16)
        for i in range(1, stripes):
            from_expert(m, i).wait_recv()
        target = got if m == 0 else backing

        def body(cols):
            source = returned[m, :, :, cols].reshape(rows, step)
            target[m, :, cols] = dot(hits, source).astype(jnp.bfloat16)

        columns(body, width, step)
        if m:
            back_copy(m).start()

    def combine(m, first, final):
        begins = plane_of(m) * rows
        share = sum(
            jnp.where(columns_ref[:, k:k + 1] - begins == low_slot, weights_ref[:, k:k + 1], 0.0)
            for k in range(TOP)
        )
        high = share.astype(jnp.bfloat16)
        low = (share - high.astype(jnp.float32)).astype(jnp.bfloat16)
        if m:
            back_copy(m).wait_recv()

        def body(cols):
            rows_got = got[m, :, cols]
            term = dot(high, rows_got) + dot(low, rows_got)
            base = hidden_ref[:, cols].astype(jnp.float32) if first else total[:, cols]
            if final:
                out_ref[:, cols] = (base + term).astype(jnp.bfloat16)
            else:
                total[:, cols] = base + term

        columns(body, width, step)

    pack(2)
    pack(1)
    out_copy(2).start()
    pack(3)
    out_copy(1).start()
    pack(0)
    out_copy(3).start()
    spread(0)
    for copy in weights[1:]:
        copy.wait()
    compute(0)
    spread(2)
    collect(0)
    combine(0, True, False)
    compute(2)
    spread(1)
    collect(2)
    compute(1)
    spread(3)
    collect(1)
    compute(3)
    collect(3)
    combine(1, False, False)
    combine(2, False, False)
    combine(3, False, True)
    for m in range(planes):
        if m:
            out_copy(m).wait_send()
            back_copy(m).wait_send()
        for i in range(1, stripes):
            to_expert(m, i).wait_send()
            from_expert(m, i).wait_send()


def mixture(capacity, stripes, slots, operands):
    mixed, stream, begin, out_weight, expert_gate, expert_up, expert_down = (
        operands[0],
        operands[1],
        operands[7],
        *operands[8:],
    )
    tok, width = stream.shape
    planes = begin.shape[0]
    vmem = pl.BlockSpec(memory_space=pltpu.VMEM)
    anywhere = pl.BlockSpec(memory_space=pl.ANY)
    dma = pltpu.SemaphoreType.DMA
    block = pltpu.VMEM((planes, capacity, width), jnp.bfloat16)
    wide = pltpu.VMEM((planes, stripes, slots, width), jnp.bfloat16)
    return pl.pallas_call(
        functools.partial(mixture_kernel, capacity, stripes, slots),
        in_specs=[vmem] * 8 + [anywhere] * 4,
        out_specs=vmem,
        out_shape=jax.ShapeDtypeStruct((tok, width), jnp.bfloat16),
        scratch_shapes=[
            pltpu.VMEM(out_weight.shape, jnp.bfloat16),
            pltpu.VMEM(expert_gate.shape[1:], jnp.bfloat16),
            pltpu.VMEM(expert_up.shape[1:], jnp.bfloat16),
            pltpu.VMEM(expert_down.shape[1:], jnp.bfloat16),
            pltpu.VMEM((tok, out_weight.shape[0]), jnp.bfloat16),
            pltpu.VMEM((tok, width), jnp.bfloat16),
            pltpu.VMEM((tok, width), jnp.bfloat16),
            block,
            block,
            wide,
            wide,
            pltpu.VMEM((stripes * slots, expert_gate.shape[2]), jnp.bfloat16),
            wide,
            wide,
            block,
            pltpu.VMEM((tok, width), jnp.float32),
            dma((4,)),
            dma((planes * stripes,)),
            dma((planes * stripes,)),
            dma((planes,)),
            dma((planes,)),
            dma((planes, stripes)),
            dma((planes, stripes)),
            dma((planes, stripes)),
            dma((planes, stripes)),
            dma((planes,)),
            dma((planes,)),
        ],
        compiler_params=pltpu.CompilerParams(
            collective_id=1 + capacity // 16,
            has_side_effects=True,
            vmem_limit_bytes=63 * 1024 * 1024,
        ),
        name="mixture",
    )(*operands)


def fast_shards(
    queries,
    keys,
    values,
    gate_totals,
    documents,
    stream,
    out_weight,
    norm_gain,
    routes,
    route_weights,
    expert_gate,
    expert_up,
    expert_down,
):
    sp_count = lax.axis_size("sp")
    group = QUERY_HEAD_COUNT // KV_HEADS
    tok = queries.shape[0]
    stripes = sp_count // KV_HEADS
    sub = tok // stripes
    blocks = 4
    span = blocks * tok
    width = min(span, 1024)
    tiles = sp_count // blocks
    slots = max(2, 2 * tok * TOP // sp_count)
    flat = jnp.transpose(routes).reshape(-1)
    hits = (flat[:, None] == jnp.arange(sp_count, dtype=jnp.int32)[None, :]).astype(jnp.int32)
    slot_index = jnp.sum(jnp.cumsum(hits, axis=0) * hits, axis=1) - 1
    own_counts = jnp.sum(hits, axis=0).reshape(KV_HEADS, stripes)
    own_offsets = jnp.cumsum(own_counts, axis=1) - own_counts
    position = (slot_index + jnp.sum(hits * own_offsets.reshape(1, -1), axis=1)).reshape(TOP, tok)
    owner = (flat // stripes).reshape(TOP, tok)
    full = stripes * slots
    place = owner * full + position
    largest = jnp.max(jnp.sum(own_counts, axis=1))
    pad = jnp.zeros((KV_HEADS, 1, tok - stripes), jnp.int32)
    told = [
        jnp.broadcast_to(documents[None, None, :], (KV_HEADS, 1, tok)),
        jnp.concatenate([own_counts[:, None, :], pad], axis=2),
        jnp.broadcast_to(largest, (KV_HEADS, 1, tok)),
        jnp.zeros((KV_HEADS, 1, tok), jnp.int32),
    ]
    notes = jnp.concatenate(
        [jnp.transpose(gate_totals).reshape(KV_HEADS, group, tok)]
        + [line.astype(jnp.float32) for line in told],
        axis=1,
    )
    kv_all, query_got, notes_all = exchange(keys, values, queries, notes, stripes)
    worst = jnp.max(notes_all[:, :, group + 2, 0]).astype(jnp.int32)
    spot = lax.rem(lax.axis_index("sp"), stripes)
    counts = lax.dynamic_index_in_dim(notes_all, spot, 0, keepdims=False)
    counts = counts[:, group + 1, :stripes].astype(jnp.int32)
    offsets = jnp.cumsum(counts, axis=1) - counts
    number = jnp.arange(slots, dtype=jnp.int32)[None, None, :]
    begin = jnp.where(number < counts[:, :, None], offsets[:, :, None] + number, -1)
    begin = begin.reshape(KV_HEADS, full)
    mixed = pl.pallas_call(
        functools.partial(attend_kernel, sub, span, width),
        grid=(tiles,),
        in_specs=[
            pl.BlockSpec((blocks, sub, group * HD), lambda i: (i, 0, 0)),
            pl.BlockSpec(kv_all.shape, lambda i: (0, 0, 0, 0)),
            pl.BlockSpec(notes_all.shape, lambda i: (0, 0, 0, 0)),
        ],
        out_specs=pl.BlockSpec((blocks, sub, group * HD), lambda i: (i, 0, 0)),
        out_shape=jax.ShapeDtypeStruct((sp_count, sub, group * HD), jnp.bfloat16),
        scratch_shapes=[pltpu.SMEM((1,), jnp.int32)],
        compiler_params=pltpu.CompilerParams(vmem_limit_bytes=48 * 1024 * 1024),
        name="attend",
    )(query_got, kv_all, notes_all)
    sizes = (full * 5 // 8, full * 11 // 16, full * 13 // 16, full)
    operands = (
        mixed,
        stream,
        norm_gain[None, :],
        place,
        jnp.transpose(place),
        route_weights,
        begin[:, None, :],
        begin[:, :, None],
        out_weight,
        expert_gate,
        expert_up,
        expert_down,
    )

    def sized(capacity):
        return lambda given: mixture(capacity, stripes, slots, given)

    choice = sum((worst > size).astype(jnp.int32) for size in sizes[:-1])
    return lax.switch(choice, [sized(size) for size in sizes], operands)


def solution(mesh):
    sp_count, tp_count = mesh.shape["sp"], mesh.shape["tp"]
    fast = tp_count == 1 and sp_count % (4 * KV_HEADS) == 0 and KV_HEADS == 4

    def body(*arrays):
        tok, stripes = arrays[0].shape[0], sp_count // KV_HEADS
        small = stripes * (2 * tok * TOP // sp_count) <= 256
        return (fast_shards if fast and small else shards)(*arrays)

    return jax.shard_map(
        body,
        mesh=mesh,
        in_specs=(
            P("sp", "tp"),
            P("sp", "tp"),
            P("sp", "tp"),
            P("sp", "tp"),
            P("sp"),
            P(("sp", "tp"), None),
            P(),
            P(),
            P(("sp", "tp"), None),
            P(("sp", "tp"), None),
            P("sp", None, "tp"),
            P("sp", None, "tp"),
            P("sp", "tp", None),
        ),
        out_specs=P(("sp", "tp"), None),
        check_vma=False,
    )
```

```python
import functools
import math

import jax
import jax.numpy as jnp
from jax import lax
from jax.experimental import pallas as pl
from jax.experimental.pallas import tpu as pltpu
from jax.sharding import PartitionSpec as P

QUERY_HEAD_COUNT = 16
KV_HEADS = 4
HD = 64
TOP = 2


EPS = 1e-06
STEP = 1024
MASKED = -1e30


def make_fold(query_rows, query_gate, key_gate_all, query_docs, first_pos, kv_local, group):
    count = query_rows.shape[0]
    scale = HD ** (-0.5)
    query_blk = query_rows.reshape(count, kv_local, group, HD)
    gate_here = query_gate.T.reshape(kv_local, group, count, 1)
    query_pos = first_pos + jnp.arange(count, dtype=jnp.int32)
    last_pos = first_pos + count - 1
    first_doc = query_docs[0]

    def block_step(carry, block_in):
        running_max, running_sum, carried = carry
        key_block, value_block, doc_block, pos_block = block_in
        width = key_block.shape[0]

        def compute(unused):
            key_heads = key_block.reshape(width, kv_local, HD)
            value_heads = value_block.reshape(width, kv_local, HD)
            gate_keys = lax.dynamic_slice_in_dim(key_gate_all, pos_block[0], width, 0).T.reshape(
                kv_local, group, 1, width
            )
            scores = (
                jnp.einsum(
                    "qkgd,nkd->kgqn", query_blk, key_heads, preferred_element_type=jnp.float32
                )
                * scale
                + gate_here
                - gate_keys
            )
            allowed = (pos_block[None, :] <= query_pos[:, None]) & (
                doc_block[None, :] == query_docs[:, None]
            )
            scores = jnp.where(allowed, scores, MASKED)
            new_max = jnp.maximum(running_max, jnp.max(scores, axis=-1))
            weights = jnp.where(allowed, jnp.exp(scores - new_max[..., None]), 0.0)
            factor = jnp.exp(running_max - new_max)
            new_sum = running_sum * factor + jnp.sum(weights, axis=-1)
            new_carried = carried * factor[..., None] + jnp.einsum(
                "kgqn,nkd->kgqd",
                weights.astype(jnp.bfloat16),
                value_heads,
                preferred_element_type=jnp.float32,
            )
            return (new_max, new_sum, new_carried)

        skipped = (pos_block[0] > last_pos) | (doc_block[width - 1] < first_doc)
        return (lax.cond(skipped, lambda unused: carry, compute, 0), None)

    def fold(carry, piece, start):
        key_piece, value_piece, doc_piece = piece
        length = key_piece.shape[0]
        width = math.gcd(length, 512)
        blocks_count = length // width
        pos_piece = jnp.arange(length, dtype=jnp.int32)
        blocks = (
            key_piece.reshape(blocks_count, width, -1),
            value_piece.reshape(blocks_count, width, -1),
            doc_piece.reshape(blocks_count, width),
            pos_piece.reshape(blocks_count, width),
        )
        carry, unused = lax.scan(block_step, carry, blocks)
        return carry

    initial = (
        jnp.full((kv_local, group, count), MASKED, jnp.float32),
        jnp.zeros((kv_local, group, count), jnp.float32),
        jnp.zeros((kv_local, group, count, HD), jnp.float32),
    )
    return (fold, initial)


def finish(running_sum, carried):
    mixed = carried / running_sum[..., None]
    count = mixed.shape[2]
    return jnp.transpose(mixed, (2, 0, 1, 3)).reshape(count, -1).astype(jnp.bfloat16)


def shards(
    queries,
    keys,
    values,
    gate_totals,
    documents,
    stream,
    out_weight,
    norm_gain,
    routes,
    route_weights,
    expert_gate,
    expert_up,
    expert_down,
):
    tp_count = lax.axis_size("tp")
    sp_count = lax.axis_size("sp")
    tp_index = lax.axis_index("tp")
    sp_index = lax.axis_index("sp")
    group = QUERY_HEAD_COUNT // KV_HEADS
    tok_local = queries.shape[0]
    own_rows = tok_local // tp_count
    first_row = sp_index * tok_local
    query_rows = lax.all_to_all(queries, "tp", split_axis=0, concat_axis=1, tiled=True)
    key_whole, value_whole = (
        lax.all_gather(keys, "tp", axis=1, tiled=True),
        lax.all_gather(values, "tp", axis=1, tiled=True),
    )
    gate_whole = lax.all_gather(gate_totals, "tp", axis=1, tiled=True)
    key_gate_all = lax.all_gather(gate_whole, "sp", axis=0, tiled=True)
    query_gate = lax.dynamic_slice_in_dim(gate_whole, tp_index * own_rows, own_rows, 0)
    query_docs = lax.dynamic_slice_in_dim(documents, tp_index * own_rows, own_rows, 0)
    fold, initial = make_fold(
        query_rows,
        query_gate,
        key_gate_all,
        query_docs,
        first_row + tp_index * own_rows,
        KV_HEADS,
        group,
    )
    running_max, running_sum, carried = fold(
        initial,
        (
            lax.all_gather(key_whole, "sp", axis=0, tiled=True),
            lax.all_gather(value_whole, "sp", axis=0, tiled=True),
            lax.all_gather(documents, "sp", axis=0, tiled=True),
        ),
        jnp.int32(0),
    )
    attended = finish(running_sum, carried)
    hidden = (
        stream.astype(jnp.float32)
        + jnp.dot(attended, out_weight, preferred_element_type=jnp.float32)
    ).astype(jnp.bfloat16)
    hidden_f = hidden.astype(jnp.float32)
    normed = (
        hidden_f
        * lax.rsqrt(jnp.mean(hidden_f * hidden_f, axis=-1, keepdims=True) + EPS)
        * norm_gain
    ).astype(jnp.bfloat16)
    local_experts = expert_gate.shape[0]
    experts_total = local_experts * sp_count
    capacity = max(2, 2 * tok_local * TOP // (tp_count * experts_total))
    flat = routes.reshape(-1)
    hits = (flat[:, None] == jnp.arange(experts_total, dtype=jnp.int32)[None, :]).astype(jnp.int32)
    slot_index = jnp.sum(jnp.cumsum(hits, axis=0) * hits, axis=1) - 1
    target = flat * capacity + slot_index
    entry_rows = jnp.repeat(normed, TOP, axis=0)
    outgoing = (
        jnp.zeros((experts_total * capacity, normed.shape[1]), jnp.bfloat16)
        .at[target]
        .set(entry_rows)
    )
    outgoing = outgoing.reshape(experts_total, capacity, -1)
    arrived = lax.all_to_all(outgoing, "sp", split_axis=0, concat_axis=0, tiled=True)
    slots = arrived.shape[1]
    both_halves = lax.all_gather(arrived, "tp", axis=0, tiled=True)
    grouped = both_halves.reshape(tp_count * sp_count, local_experts, slots, -1)
    gate = jnp.einsum("secd,edf->secf", grouped, expert_gate, preferred_element_type=jnp.float32)
    upper = jnp.einsum("secd,edf->secf", grouped, expert_up, preferred_element_type=jnp.float32)
    inner = (jax.nn.silu(gate) * upper).astype(jnp.bfloat16)
    partial_value = jnp.einsum(
        "secf,efd->secd", inner, expert_down, preferred_element_type=jnp.float32
    )
    partial_value = lax.optimization_barrier(partial_value.astype(jnp.bfloat16)).astype(jnp.float32)
    summed = lax.psum_scatter(
        partial_value.reshape(tp_count * sp_count * local_experts, slots, -1).astype(jnp.bfloat16),
        "tp",
        scatter_dimension=0,
        tiled=True,
    )
    returned = lax.all_to_all(summed, "sp", split_axis=0, concat_axis=0, tiled=True)
    answers = returned.reshape(experts_total * capacity, -1)[target].reshape(own_rows, TOP, -1)
    routed = jnp.sum(route_weights[..., None] * answers.astype(jnp.float32), axis=1)
    return (hidden_f + routed).astype(jnp.bfloat16)


def attend_kernel(sub, span, width, query_ref, kv_ref, notes_ref, out_ref, boundary_ref):
    tile = pl.program_id(0)
    stripes = kv_ref.shape[0]
    stripe = lax.rem(lax.axis_index("sp"), stripes)
    blocks = query_ref.shape[0]
    block = span // blocks
    group = QUERY_HEAD_COUNT // KV_HEADS
    rows = blocks * sub

    @pl.when(tile == 0)
    def count():
        earlier = notes_ref[:, :, group:group + 1, :] < 0.5
        boundary_ref[0] = jnp.sum(earlier.astype(jnp.float32)).astype(jnp.int32)

    boundary = boundary_ref[0]
    first = tile * span
    per_tile = span // width
    taken = width // block
    zeros = jnp.zeros((rows, HD), jnp.bfloat16)
    query = query_ref[...].reshape(rows, group * HD) * jnp.bfloat16(HD ** (-0.5))
    stacked = jnp.concatenate(
        [
            jnp.concatenate([query[:, head * HD:(head + 1) * HD], zeros], axis=1)
            for head in range(group)
        ],
        axis=0,
    )
    row = lax.broadcasted_iota(jnp.int32, (rows, 1), 0)
    query_pos = first + (row // sub) * block + stripe * sub + lax.rem(row, sub)
    doc_start = jnp.where(query_pos >= boundary, boundary, 0)
    per_z = stripes // taken

    def gate_rows(index):
        block_notes = notes_ref[pl.ds(lax.rem(index, per_z) * taken, taken), index // per_z]
        return [
            jnp.concatenate(
                [block_notes[at, head:head + 1, :] for at in range(taken)], axis=1
            )
            for head in range(group)
        ]

    origin = [gate[:, 0:1] for gate in gate_rows(tile * per_tile)]
    lane = lax.broadcasted_iota(jnp.int32, (width, 2 * HD), 1)

    def chunk(index, carry, masked):
        kv = kv_ref[pl.ds(lax.rem(index, per_z) * taken, taken), index // per_z]
        kv = kv.reshape(width, 2 * HD)
        bias = [start - gate for start, gate in zip(origin, gate_rows(index))]
        if masked:
            key_pos = index * width + lax.broadcasted_iota(jnp.int32, (1, width), 1)
            allowed = (key_pos <= query_pos) & (key_pos >= doc_start)
        scores = lax.dot_general(
            stacked, kv, (((1,), (1,)), ((), ())), preferred_element_type=jnp.float32
        )
        tops, mixed = carry
        new_tops, factors, weights = [], [], []
        for head in range(group):
            score = scores[head * rows:(head + 1) * rows] + bias[head]
            if masked:
                score = jnp.where(allowed, score, MASKED)
            new_top = jnp.maximum(tops[head], jnp.max(score, axis=1, keepdims=True))
            weight = jnp.exp(score - new_top)
            factor = jnp.exp(tops[head] - new_top)
            new_tops.append(new_top)
            factors.append(factor)
            weights.append(weight.astype(jnp.bfloat16))
        mixed = mixed * jnp.concatenate(factors, axis=0) + jnp.dot(
            jnp.concatenate(weights, axis=0),
            jnp.where(lane < HD, jnp.bfloat16(1), kv),
            preferred_element_type=jnp.float32,
        )
        return (tuple(new_tops), mixed)

    carry = (
        tuple(jnp.full((rows, 1), 0.5 * MASKED, jnp.float32) for unused in range(group)),
        jnp.zeros((group * rows, 2 * HD), jnp.float32),
    )
    own = tile * per_tile
    inside = (boundary > first) & (boundary < first + span)
    second = first >= boundary
    low = jnp.where(second, boundary // width, 0)
    clean_low = jnp.where(inside, own, jnp.where(second, (boundary + width - 1) // width, 0))
    clean_low = jnp.minimum(clean_low, own)
    carry = lax.fori_loop(low, clean_low, lambda i, c: chunk(i, c, True), carry)
    carry = lax.fori_loop(clean_low, own, lambda i, c: chunk(i, c, False), carry)
    carry = lax.fori_loop(own, own + per_tile, lambda i, c: chunk(i, c, True), carry)
    unused, mixed = carry
    ratio = mixed[:, HD:] / mixed[:, :HD]
    parts = [ratio[head * rows:(head + 1) * rows] for head in range(group)]
    out_ref[...] = jnp.concatenate(parts, axis=1).astype(jnp.bfloat16).reshape(out_ref.shape)


def exchange_kernel(
    stripes,
    keys_hbm,
    values_hbm,
    query_ref,
    notes_ref,
    kv_all_ref,
    got_ref,
    notes_all_ref,
    keys_ref,
    values_ref,
    kv_ref,
    l_sem,
    z_send,
    z_recv,
    p_send,
    p_recv,
    s_send,
    s_recv,
    q_send,
    q_recv,
):
    total, sub, wide = got_ref.shape
    planes = total // stripes
    chips = stripes // 2
    me = lax.axis_index("sp")
    plane, spot = me // stripes, lax.rem(me, stripes)
    chip, core = spot // 2, lax.rem(spot, 2)
    partner = plane * stripes + chip * 2 + (1 - core)
    barrier = pltpu.get_barrier_semaphore()

    def piece(other):
        head, stripe = other // stripes, lax.rem(other, stripes)
        return (
            pl.ds(pl.multiple_of(stripe * sub, sub), sub),
            pl.ds(pl.multiple_of(head * wide, wide), wide),
        )

    def greet(r, carry):
        pl.semaphore_signal(barrier, inc=1, device_id={"sp": lax.rem(me + r, total)})
        return carry

    lax.fori_loop(1, total, greet, 0)
    loads = [
        pltpu.make_async_copy(keys_hbm, keys_ref, l_sem.at[0]),
        pltpu.make_async_copy(values_hbm, values_ref, l_sem.at[1]),
        pltpu.make_async_copy(query_ref.at[piece(me)], got_ref.at[me], l_sem.at[2]),
    ]
    for load in loads:
        load.start()
    for load in loads[:2]:
        load.wait()
    for g in range(planes):
        part = slice(g * HD, (g + 1) * HD)
        kv_ref[g] = jnp.concatenate([keys_ref[:, part], values_ref[:, part]], axis=1)
    pl.semaphore_wait(barrier, total - 1)
    sources, targets = (kv_ref, notes_ref), (kv_all_ref, notes_all_ref)

    def along(r, n):
        other = lax.rem(plane + r, planes)
        return pltpu.make_async_remote_copy(
            src_ref=sources[n].at[other],
            dst_ref=targets[n].at[spot, plane],
            send_sem=z_send.at[n, r],
            recv_sem=z_recv.at[n, r],
            device_id={"sp": other * stripes + spot},
        )

    def origin(r):
        return lax.rem(plane + planes - r, planes)

    def block(r, n):
        if r == 0:
            return sources[n].at[plane]
        return targets[n].at[spot, origin(r)]

    def across(r, m, n):
        target = lax.rem(chip + m, chips)
        return pltpu.make_async_remote_copy(
            src_ref=block(r, n),
            dst_ref=targets[n].at[spot, origin(r)],
            send_sem=p_send.at[n, r, m],
            recv_sem=p_recv.at[n, r, m],
            device_id={"sp": plane * stripes + target * 2 + core},
        )

    def over(r, m, n):
        source = lax.rem(chip + chips - m, chips) * 2 + core
        where = targets[n].at[source, origin(r)]
        return pltpu.make_async_remote_copy(
            src_ref=block(r, n) if m == 0 else where,
            dst_ref=where,
            send_sem=s_send.at[n, r, m],
            recv_sem=s_recv.at[n, r, m],
            device_id={"sp": partner},
        )

    def direct(r):
        other = lax.rem(me + r, total)
        return pltpu.make_async_remote_copy(
            src_ref=query_ref.at[piece(other)],
            dst_ref=got_ref.at[me],
            send_sem=q_send.at[r],
            recv_sem=q_recv.at[r],
            device_id={"sp": other},
        )

    both = (0, 1)
    order = sorted(range(1, planes), key=lambda r: min(r, planes - r))
    for r in order:
        for n in both:
            along(r, n).start()
    for m in range(1, chips):
        for n in both:
            across(0, m, n).start()
    for n in both:
        over(0, 0, n).start()

    def send_query(r, carry):
        direct(r).start()
        return carry

    lax.fori_loop(1, total, send_query, 0)
    kv_all_ref[spot, plane] = kv_ref[plane]
    notes_all_ref[spot, plane] = notes_ref[plane]
    loads[2].wait()
    for at, r in enumerate(order):
        for n in both:
            along(r, n).wait_recv()
            for m in range(1, chips):
                across(r, m, n).start()
            over(r, 0, n).start()
        earlier = 0 if at == 0 else order[at - 1]
        for m in range(1, chips):
            for n in both:
                across(earlier, m, n).wait_recv()
                over(earlier, m, n).start()
    for m in range(1, chips):
        for n in both:
            across(order[-1], m, n).wait_recv()
            over(order[-1], m, n).start()
    for n in both:
        for r in range(planes):
            for m in range(chips):
                over(r, m, n).wait()
        for r in range(1, planes):
            along(r, n).wait_send()
        for r in range(planes):
            for m in range(1, chips):
                across(r, m, n).wait_send()

    def end_query(r, carry):
        direct(r).wait()
        return carry

    lax.fori_loop(1, total, end_query, 0)


def exchange(keys, values, queries, notes, stripes):
    planes, chips = notes.shape[0], stripes // 2
    total, tok = planes * stripes, keys.shape[0]
    got = (total, tok // stripes, queries.shape[1] // planes)
    hbm = pl.BlockSpec(memory_space=pltpu.HBM)
    vmem = pl.BlockSpec(memory_space=pltpu.VMEM)
    dma = pltpu.SemaphoreType.DMA
    return pl.pallas_call(
        functools.partial(exchange_kernel, stripes),
        in_specs=[hbm, hbm, hbm, vmem],
        out_specs=[vmem] * 3,
        out_shape=[
            jax.ShapeDtypeStruct((stripes, planes, tok, 2 * HD), keys.dtype),
            jax.ShapeDtypeStruct(got, queries.dtype),
            jax.ShapeDtypeStruct((stripes,) + notes.shape, notes.dtype),
        ],
        scratch_shapes=[
            pltpu.VMEM(keys.shape, keys.dtype),
            pltpu.VMEM(values.shape, values.dtype),
            pltpu.VMEM((planes, tok, 2 * HD), keys.dtype),
            dma((3,)),
            dma((2, planes)),
            dma((2, planes)),
            dma((2, planes, chips)),
            dma((2, planes, chips)),
            dma((2, planes, chips)),
            dma((2, planes, chips)),
            dma((total,)),
            dma((total,)),
        ],
        compiler_params=pltpu.CompilerParams(
            collective_id=0, has_side_effects=True, vmem_limit_bytes=24 * 1024 * 1024
        ),
        name="exchange",
    )(keys, values, queries, notes)


def mixture_kernel(
    capacity,
    stripes,
    slots,
    mixed_ref,
    gain_ref,
    rows_ref,
    columns_ref,
    begin_row_ref,
    begin_ref,
    stream_hbm,
    weights_hbm,
    project_hbm,
    gate_hbm,
    up_hbm,
    down_hbm,
    out_ref,
    stream_ref,
    weights_ref,
    project_w,
    gate_w,
    up_w,
    down_w,
    attended,
    hidden_ref,
    normed_ref,
    packed,
    landed,
    sending,
    arrived,
    inner,
    answers,
    returned,
    got,
    total,
    w_sem,
    h_send,
    h_recv,
    z_send,
    z_recv,
    a_send,
    a_recv,
    b_send,
    b_recv,
    r_send,
    r_recv,
):
    planes = begin_ref.shape[0]
    devices = planes * stripes
    tok, width = stream_ref.shape
    sub, wide = mixed_ref.shape[1:]
    backing = landed
    hidden_units = gate_w.shape[1]
    rows = stripes * slots
    step = math.gcd(width, STEP)
    me = lax.axis_index("sp")
    plane, spot = me // stripes, lax.rem(me, stripes)

    def plane_of(m):
        return 2 * lax.rem(plane // 2 + m // 2, 2) + lax.rem(plane + m, 2)

    def turned(q):
        return 2 * lax.rem((q + 1) // 2, 2) + q // 2

    barrier = pltpu.get_barrier_semaphore()

    def greet(r, carry):
        pl.semaphore_signal(barrier, inc=1, device_id={"sp": lax.rem(me + r, devices)})
        return carry

    lax.fori_loop(1, devices, greet, 0)
    weights = [
        pltpu.make_async_copy(source, target, w_sem.at[at])
        for at, (source, target) in enumerate(
            (
                (stream_hbm, stream_ref),
                (weights_hbm, weights_ref),
                (project_hbm, project_w),
                (gate_hbm.at[0], gate_w),
                (up_hbm.at[0], up_w),
                (down_hbm.at[0], down_w),
            )
        )
    ]
    for copy in weights:
        copy.start()
    pl.semaphore_wait(barrier, devices - 1)

    def home(owner):
        head, stripe = owner // stripes, lax.rem(owner, stripes)
        return (
            pl.ds(pl.multiple_of(stripe * sub, sub), sub),
            pl.ds(pl.multiple_of(head * wide, wide), wide),
        )

    def home_copy(r):
        other = lax.rem(me + r, devices)
        return pltpu.make_async_remote_copy(
            src_ref=mixed_ref.at[other],
            dst_ref=attended.at[home(me)],
            send_sem=h_send.at[r],
            recv_sem=h_recv.at[r],
            device_id={"sp": other},
        )

    def send_home(r, carry):
        home_copy(r).start()
        return carry

    def wait_home(r, carry):
        home_copy(r).wait()
        return carry

    lax.fori_loop(1, devices, send_home, 0)
    attended[home(me)] = mixed_ref[me]
    lax.fori_loop(1, devices, wait_home, 0)
    for copy in weights[:3]:
        copy.wait()

    def project(index, squares):
        cols = pl.ds(pl.multiple_of(index * step, step), step)
        product = jnp.dot(attended[...], project_w[:, cols], preferred_element_type=jnp.float32)
        hidden = (stream_ref[:, cols].astype(jnp.float32) + product).astype(jnp.bfloat16)
        hidden_ref[:, cols] = hidden
        wider = hidden.astype(jnp.float32)
        total[:, cols] = wider
        return squares + jnp.sum(wider * wider, axis=1, keepdims=True)

    squares = lax.fori_loop(0, width // step, project, jnp.zeros((tok, 1), jnp.float32))
    inverse = lax.rsqrt(squares / width + EPS)

    def columns(body, length, size):
        def at(index, carry):
            body(pl.ds(pl.multiple_of(index * size, size), size))
            return carry

        lax.fori_loop(0, length // size, at, 0)

    def dot(left, right):
        return jnp.dot(left, right, preferred_element_type=jnp.float32)

    def norm(cols):
        scaled = hidden_ref[:, cols].astype(jnp.float32) * inverse * gain_ref[:, cols]
        normed_ref[:, cols] = scaled.astype(jnp.bfloat16)

    columns(norm, width, step)
    high_slot = lax.broadcasted_iota(jnp.int32, (capacity, 1), 0)
    low_slot = lax.broadcasted_iota(jnp.int32, (1, capacity), 1)

    def chosen_of(hit):
        return jnp.where(hit, 1.0, 0.0)

    def out_copy(m):
        return pltpu.make_async_remote_copy(
            src_ref=packed.at[m],
            dst_ref=landed.at[m],
            send_sem=z_send.at[m],
            recv_sem=z_recv.at[m],
            device_id={"sp": plane_of(m) * stripes + spot},
        )

    def back_copy(m):
        return pltpu.make_async_remote_copy(
            src_ref=backing.at[m],
            dst_ref=got.at[m],
            send_sem=r_send.at[m],
            recv_sem=r_recv.at[m],
            device_id={"sp": plane_of(m) * stripes + spot},
        )

    def near_copy(source, target, send, recv, m, i):
        other = lax.rem(spot + i, stripes)
        return pltpu.make_async_remote_copy(
            src_ref=source.at[m, other],
            dst_ref=target.at[m, spot],
            send_sem=send.at[m, i],
            recv_sem=recv.at[m, i],
            device_id={"sp": plane * stripes + other},
        )

    def to_expert(m, i):
        return near_copy(sending, arrived, a_send, a_recv, m, i)

    def from_expert(m, i):
        return near_copy(answers, returned, b_send, b_recv, m, i)

    def pack(m):
        begins = plane_of(m) * rows
        hits = sum(chosen_of(rows_ref[k:k + 1] - begins == high_slot) for k in range(TOP))
        hits = hits.astype(jnp.bfloat16)

        def body(cols):
            packed[m, :, cols] = dot(hits, normed_ref[:, cols]).astype(jnp.bfloat16)

        columns(body, width, step)

    def peers(act):
        def at(i, carry):
            act(i)
            return carry

        lax.fori_loop(1, stripes, at, 0)

    def spread(m):
        hits = chosen_of(begin_ref[plane_of(m)] == low_slot).astype(jnp.bfloat16)

        @pl.when(m > 0)
        def wait():
            out_copy(m).wait_recv()

        def body(cols):
            chosen = dot(hits, landed[m, :, cols]).astype(jnp.bfloat16)
            sending[m, :, :, cols] = chosen.reshape(stripes, slots, step)

        columns(body, width, step)
        arrived[m, spot] = sending[m, spot]
        peers(lambda i: to_expert(m, i).start())

    def take(m):
        peers(lambda i: to_expert(m, i).wait_recv())

    def compute(m):
        def middle(cols):
            rows_in = arrived[m].reshape(rows, width)
            gate = dot(rows_in, gate_w[:, cols])
            upper = dot(rows_in, up_w[:, cols])
            inner[:, cols] = (jax.nn.silu(gate) * upper).astype(jnp.bfloat16)

        columns(middle, hidden_units, math.gcd(hidden_units, 256))

        def last(cols):
            answer = dot(inner[...], down_w[:, cols]).astype(jnp.bfloat16)
            answers[m, :, :, cols] = answer.reshape(stripes, slots, step)

        columns(last, width, step)
        returned[m, spot] = answers[m, spot]
        peers(lambda i: from_expert(m, i).start())

    def collect(m):
        hits = chosen_of(begin_row_ref[plane_of(m)] == high_slot).astype(jnp.bfloat16)
        peers(lambda i: from_expert(m, i).wait_recv())

        def body(cols):
            source = returned[m, :, :, cols].reshape(rows, step)
            backing[m, :, cols] = dot(hits, source).astype(jnp.bfloat16)

        columns(body, width, step)

        @pl.when(m > 0)
        def send():
            back_copy(m).start()

    def combine(m, final):
        begins = plane_of(m) * rows
        share = sum(
            jnp.where(columns_ref[:, k:k + 1] - begins == low_slot, weights_ref[:, k:k + 1], 0.0)
            for k in range(TOP)
        )
        high = share.astype(jnp.bfloat16)
        low = (share - high.astype(jnp.float32)).astype(jnp.bfloat16)

        def body(cols):
            rows_got = got[m, :, cols]
            term = total[:, cols] + dot(high, rows_got) + dot(low, rows_got)
            if final:
                out_ref[:, cols] = term.astype(jnp.bfloat16)
            else:
                total[:, cols] = term

        columns(body, width, step)

    def far_first(q):
        return 2 * lax.rem(q + 1, 2) + lax.rem((q + 1) // 2, 2)

    def fill(q, carry):
        pack(far_first(q))

        @pl.when(q > 0)
        def send():
            out_copy(far_first(q - 1)).start()

        return carry

    lax.fori_loop(0, planes, fill, 0)
    landed[0] = packed[0]

    def work(q, carry):
        @pl.when((q > 0) & (q != 3))
        def first():
            collect(turned(q - 1 - q // 4))

        @pl.when(q < 3)
        def second():
            def at(extra, inner_carry):
                spread(turned(q + extra))
                take_now = turned(q)

                @pl.when(extra == 0)
                def third():
                    take(take_now)

                return inner_carry

            lax.fori_loop(0, 1 + q // 2, at, 0)

        @pl.when(q == 0)
        def ready():
            for copy in weights[3:]:
                copy.wait()

        @pl.when(q == 3)
        def last():
            take(turned(q))

        @pl.when(q < planes)
        def fourth():
            compute(turned(q))

        return carry

    lax.fori_loop(0, planes + 2, work, 0)
    got[0] = backing[0]

    def gather(q, carry):
        m = turned(q)

        @pl.when(m > 0)
        def wait():
            back_copy(m).wait_recv()

        combine(m, False)
        return carry

    lax.fori_loop(0, planes - 1, gather, 0)
    back_copy(1).wait_recv()
    combine(1, True)

    def finish_sends(m, carry):
        @pl.when(m > 0)
        def far():
            out_copy(m).wait_send()
            back_copy(m).wait_send()

        peers(lambda i: to_expert(m, i).wait_send())
        peers(lambda i: from_expert(m, i).wait_send())
        return carry

    lax.fori_loop(0, planes, finish_sends, 0)


def mixture(capacity, stripes, slots, operands):
    begin = operands[5]
    stream, route_weights, out_weight, expert_gate, expert_up, expert_down = operands[6:]
    tok, width = stream.shape
    planes = begin.shape[0]
    vmem = pl.BlockSpec(memory_space=pltpu.VMEM)
    hbm = pl.BlockSpec(memory_space=pltpu.HBM)
    dma = pltpu.SemaphoreType.DMA
    block = pltpu.VMEM((planes, capacity, width), jnp.bfloat16)
    wide = pltpu.VMEM((planes, stripes, slots, width), jnp.bfloat16)
    return pl.pallas_call(
        functools.partial(mixture_kernel, capacity, stripes, slots),
        in_specs=[vmem] * 6 + [hbm] * 6,
        out_specs=vmem,
        out_shape=jax.ShapeDtypeStruct((tok, width), jnp.bfloat16),
        scratch_shapes=[
            pltpu.VMEM(stream.shape, stream.dtype),
            pltpu.VMEM(route_weights.shape, route_weights.dtype),
            pltpu.VMEM(out_weight.shape, jnp.bfloat16),
            pltpu.VMEM(expert_gate.shape[1:], jnp.bfloat16),
            pltpu.VMEM(expert_up.shape[1:], jnp.bfloat16),
            pltpu.VMEM(expert_down.shape[1:], jnp.bfloat16),
            pltpu.VMEM((tok, out_weight.shape[0]), jnp.bfloat16),
            pltpu.VMEM((tok, width), jnp.bfloat16),
            pltpu.VMEM((tok, width), jnp.bfloat16),
            block,
            block,
            wide,
            wide,
            pltpu.VMEM((stripes * slots, expert_gate.shape[2]), jnp.bfloat16),
            wide,
            wide,
            block,
            pltpu.VMEM((tok, width), jnp.float32),
            dma((6,)),
            dma((planes * stripes,)),
            dma((planes * stripes,)),
            dma((planes,)),
            dma((planes,)),
            dma((planes, stripes)),
            dma((planes, stripes)),
            dma((planes, stripes)),
            dma((planes, stripes)),
            dma((planes,)),
            dma((planes,)),
        ],
        compiler_params=pltpu.CompilerParams(
            collective_id=1 + capacity // 16,
            has_side_effects=True,
            vmem_limit_bytes=63 * 1024 * 1024,
        ),
        name="mixture",
    )(*operands)


def fast_shards(
    queries,
    keys,
    values,
    gate_totals,
    documents,
    stream,
    out_weight,
    norm_gain,
    routes,
    route_weights,
    expert_gate,
    expert_up,
    expert_down,
):
    sp_count = lax.axis_size("sp")
    group = QUERY_HEAD_COUNT // KV_HEADS
    tok = queries.shape[0]
    stripes = sp_count // KV_HEADS
    sub = tok // stripes
    blocks = 4
    span = blocks * tok
    width = min(span, 1024)
    tiles = sp_count // blocks
    slots = max(2, 2 * tok * TOP // sp_count)
    flat = jnp.transpose(routes).reshape(-1)
    hits = (flat[:, None] == jnp.arange(sp_count, dtype=jnp.int32)[None, :]).astype(jnp.int32)
    slot_index = jnp.sum(jnp.cumsum(hits, axis=0) * hits, axis=1) - 1
    own_counts = jnp.sum(hits, axis=0).reshape(KV_HEADS, stripes)
    below = jnp.arange(stripes)[None, :, None] < jnp.arange(stripes)[None, None, :]
    own_offsets = jnp.sum(jnp.where(below, own_counts[:, :, None], 0), axis=1)
    position = (slot_index + jnp.sum(hits * own_offsets.reshape(1, -1), axis=1)).reshape(TOP, tok)
    owner = (flat // stripes).reshape(TOP, tok)
    full = stripes * slots
    place = owner * full + position
    largest = jnp.max(jnp.sum(own_counts, axis=1))
    pad = jnp.zeros((KV_HEADS, 1, tok - stripes), jnp.int32)
    told = [
        jnp.broadcast_to(documents[None, None, :], (KV_HEADS, 1, tok)),
        jnp.concatenate([own_counts[:, None, :], pad], axis=2),
        jnp.broadcast_to(largest, (KV_HEADS, 1, tok)),
        jnp.zeros((KV_HEADS, 1, tok), jnp.int32),
    ]
    notes = jnp.concatenate(
        [jnp.transpose(gate_totals).reshape(KV_HEADS, group, tok)]
        + [line.astype(jnp.float32) for line in told],
        axis=1,
    )
    kv_all, query_got, notes_all = exchange(keys, values, queries, notes, stripes)
    worst = jnp.max(notes_all[:, :, group + 2, 0]).astype(jnp.int32)
    spot = lax.rem(lax.axis_index("sp"), stripes)
    counts = lax.dynamic_index_in_dim(notes_all, spot, 0, keepdims=False)
    counts = counts[:, group + 1, :stripes].astype(jnp.int32)
    offsets = jnp.sum(jnp.where(below, counts[:, :, None], 0), axis=1)
    number = jnp.arange(slots, dtype=jnp.int32)[None, None, :]
    begin = jnp.where(number < counts[:, :, None], offsets[:, :, None] + number, -1)
    begin = begin.reshape(KV_HEADS, full)
    mixed = pl.pallas_call(
        functools.partial(attend_kernel, sub, span, width),
        grid=(tiles,),
        in_specs=[
            pl.BlockSpec((blocks, sub, group * HD), lambda i: (i, 0, 0)),
            pl.BlockSpec(kv_all.shape, lambda i: (0, 0, 0, 0)),
            pl.BlockSpec(notes_all.shape, lambda i: (0, 0, 0, 0)),
        ],
        out_specs=pl.BlockSpec((blocks, sub, group * HD), lambda i: (i, 0, 0)),
        out_shape=jax.ShapeDtypeStruct((sp_count, sub, group * HD), jnp.bfloat16),
        scratch_shapes=[pltpu.SMEM((1,), jnp.int32)],
        compiler_params=pltpu.CompilerParams(vmem_limit_bytes=48 * 1024 * 1024),
        name="attend",
    )(query_got, kv_all, notes_all)
    sizes = tuple(full * part // 32 for part in (20, 22, 24, 32))
    operands = (
        mixed,
        norm_gain[None, :],
        place,
        jnp.transpose(place),
        begin[:, None, :],
        begin[:, :, None],
        stream,
        route_weights,
        out_weight,
        expert_gate,
        expert_up,
        expert_down,
    )

    def sized(capacity):
        return lambda given: mixture(capacity, stripes, slots, given)

    choice = sum((worst > size).astype(jnp.int32) for size in sizes[:-1])
    return lax.switch(choice, [sized(size) for size in sizes], operands)


def solution(mesh):
    sp_count, tp_count = mesh.shape["sp"], mesh.shape["tp"]
    fast = tp_count == 1 and sp_count % (4 * KV_HEADS) == 0 and KV_HEADS == 4

    def body(*arrays):
        tok, stripes = arrays[0].shape[0], sp_count // KV_HEADS
        small = stripes * (2 * tok * TOP // sp_count) <= 256
        return (fast_shards if fast and small else shards)(*arrays)

    return jax.shard_map(
        body,
        mesh=mesh,
        in_specs=(
            P("sp", "tp"),
            P("sp", "tp"),
            P("sp", "tp"),
            P("sp", "tp"),
            P("sp"),
            P(("sp", "tp"), None),
            P(),
            P(),
            P(("sp", "tp"), None),
            P(("sp", "tp"), None),
            P("sp", None, "tp"),
            P("sp", None, "tp"),
            P("sp", "tp", None),
        ),
        out_specs=P(("sp", "tp"), None),
        check_vma=False,
    )
```

```python
import functools
import math

import jax
import jax.numpy as jnp
from jax import lax
from jax.experimental import pallas as pl
from jax.experimental.pallas import tpu as pltpu
from jax.sharding import PartitionSpec as P

QUERY_HEAD_COUNT = 16
KV_HEADS = 4
HD = 64
TOP = 2


EPS = 1e-06
STEP = 1024
MASKED = -1e30


def make_fold(query_rows, query_gate, key_gate_all, query_docs, first_pos, kv_local, group):
    count = query_rows.shape[0]
    scale = HD ** (-0.5)
    query_blk = query_rows.reshape(count, kv_local, group, HD)
    gate_here = query_gate.T.reshape(kv_local, group, count, 1)
    query_pos = first_pos + jnp.arange(count, dtype=jnp.int32)
    last_pos = first_pos + count - 1
    first_doc = query_docs[0]

    def block_step(carry, block_in):
        running_max, running_sum, carried = carry
        key_block, value_block, doc_block, pos_block = block_in
        width = key_block.shape[0]

        def compute(unused):
            key_heads = key_block.reshape(width, kv_local, HD)
            value_heads = value_block.reshape(width, kv_local, HD)
            gate_keys = lax.dynamic_slice_in_dim(key_gate_all, pos_block[0], width, 0).T.reshape(
                kv_local, group, 1, width
            )
            scores = (
                jnp.einsum(
                    "qkgd,nkd->kgqn", query_blk, key_heads, preferred_element_type=jnp.float32
                )
                * scale
                + gate_here
                - gate_keys
            )
            allowed = (pos_block[None, :] <= query_pos[:, None]) & (
                doc_block[None, :] == query_docs[:, None]
            )
            scores = jnp.where(allowed, scores, MASKED)
            new_max = jnp.maximum(running_max, jnp.max(scores, axis=-1))
            weights = jnp.where(allowed, jnp.exp(scores - new_max[..., None]), 0.0)
            factor = jnp.exp(running_max - new_max)
            new_sum = running_sum * factor + jnp.sum(weights, axis=-1)
            new_carried = carried * factor[..., None] + jnp.einsum(
                "kgqn,nkd->kgqd",
                weights.astype(jnp.bfloat16),
                value_heads,
                preferred_element_type=jnp.float32,
            )
            return (new_max, new_sum, new_carried)

        skipped = (pos_block[0] > last_pos) | (doc_block[width - 1] < first_doc)
        return (lax.cond(skipped, lambda unused: carry, compute, 0), None)

    def fold(carry, piece, start):
        key_piece, value_piece, doc_piece = piece
        length = key_piece.shape[0]
        width = math.gcd(length, 512)
        blocks_count = length // width
        pos_piece = jnp.arange(length, dtype=jnp.int32)
        blocks = (
            key_piece.reshape(blocks_count, width, -1),
            value_piece.reshape(blocks_count, width, -1),
            doc_piece.reshape(blocks_count, width),
            pos_piece.reshape(blocks_count, width),
        )
        carry, unused = lax.scan(block_step, carry, blocks)
        return carry

    initial = (
        jnp.full((kv_local, group, count), MASKED, jnp.float32),
        jnp.zeros((kv_local, group, count), jnp.float32),
        jnp.zeros((kv_local, group, count, HD), jnp.float32),
    )
    return (fold, initial)


def finish(running_sum, carried):
    mixed = carried / running_sum[..., None]
    count = mixed.shape[2]
    return jnp.transpose(mixed, (2, 0, 1, 3)).reshape(count, -1).astype(jnp.bfloat16)


def shards(
    queries,
    keys,
    values,
    gate_totals,
    documents,
    stream,
    out_weight,
    norm_gain,
    routes,
    route_weights,
    expert_gate,
    expert_up,
    expert_down,
):
    tp_count = lax.axis_size("tp")
    sp_count = lax.axis_size("sp")
    tp_index = lax.axis_index("tp")
    sp_index = lax.axis_index("sp")
    group = QUERY_HEAD_COUNT // KV_HEADS
    tok_local = queries.shape[0]
    own_rows = tok_local // tp_count
    first_row = sp_index * tok_local
    query_rows = lax.all_to_all(queries, "tp", split_axis=0, concat_axis=1, tiled=True)
    key_whole, value_whole = (
        lax.all_gather(keys, "tp", axis=1, tiled=True),
        lax.all_gather(values, "tp", axis=1, tiled=True),
    )
    gate_whole = lax.all_gather(gate_totals, "tp", axis=1, tiled=True)
    key_gate_all = lax.all_gather(gate_whole, "sp", axis=0, tiled=True)
    query_gate = lax.dynamic_slice_in_dim(gate_whole, tp_index * own_rows, own_rows, 0)
    query_docs = lax.dynamic_slice_in_dim(documents, tp_index * own_rows, own_rows, 0)
    fold, initial = make_fold(
        query_rows,
        query_gate,
        key_gate_all,
        query_docs,
        first_row + tp_index * own_rows,
        KV_HEADS,
        group,
    )
    running_max, running_sum, carried = fold(
        initial,
        (
            lax.all_gather(key_whole, "sp", axis=0, tiled=True),
            lax.all_gather(value_whole, "sp", axis=0, tiled=True),
            lax.all_gather(documents, "sp", axis=0, tiled=True),
        ),
        jnp.int32(0),
    )
    attended = finish(running_sum, carried)
    hidden = (
        stream.astype(jnp.float32)
        + jnp.dot(attended, out_weight, preferred_element_type=jnp.float32)
    ).astype(jnp.bfloat16)
    hidden_f = hidden.astype(jnp.float32)
    normed = (
        hidden_f
        * lax.rsqrt(jnp.mean(hidden_f * hidden_f, axis=-1, keepdims=True) + EPS)
        * norm_gain
    ).astype(jnp.bfloat16)
    local_experts = expert_gate.shape[0]
    experts_total = local_experts * sp_count
    capacity = max(2, 2 * tok_local * TOP // (tp_count * experts_total))
    flat = routes.reshape(-1)
    hits = (flat[:, None] == jnp.arange(experts_total, dtype=jnp.int32)[None, :]).astype(jnp.int32)
    slot_index = jnp.sum(jnp.cumsum(hits, axis=0) * hits, axis=1) - 1
    target = flat * capacity + slot_index
    entry_rows = jnp.repeat(normed, TOP, axis=0)
    outgoing = (
        jnp.zeros((experts_total * capacity, normed.shape[1]), jnp.bfloat16)
        .at[target]
        .set(entry_rows)
    )
    outgoing = outgoing.reshape(experts_total, capacity, -1)
    arrived = lax.all_to_all(outgoing, "sp", split_axis=0, concat_axis=0, tiled=True)
    slots = arrived.shape[1]
    both_halves = lax.all_gather(arrived, "tp", axis=0, tiled=True)
    grouped = both_halves.reshape(tp_count * sp_count, local_experts, slots, -1)
    gate = jnp.einsum("secd,edf->secf", grouped, expert_gate, preferred_element_type=jnp.float32)
    upper = jnp.einsum("secd,edf->secf", grouped, expert_up, preferred_element_type=jnp.float32)
    inner = (jax.nn.silu(gate) * upper).astype(jnp.bfloat16)
    partial_value = jnp.einsum(
        "secf,efd->secd", inner, expert_down, preferred_element_type=jnp.float32
    )
    partial_value = lax.optimization_barrier(partial_value.astype(jnp.bfloat16)).astype(jnp.float32)
    summed = lax.psum_scatter(
        partial_value.reshape(tp_count * sp_count * local_experts, slots, -1).astype(jnp.bfloat16),
        "tp",
        scatter_dimension=0,
        tiled=True,
    )
    returned = lax.all_to_all(summed, "sp", split_axis=0, concat_axis=0, tiled=True)
    answers = returned.reshape(experts_total * capacity, -1)[target].reshape(own_rows, TOP, -1)
    routed = jnp.sum(route_weights[..., None] * answers.astype(jnp.float32), axis=1)
    return (hidden_f + routed).astype(jnp.bfloat16)


def attend_kernel(sub, span, width, query_ref, kv_ref, notes_ref, out_ref, boundary_ref):
    tile = pl.program_id(0)
    stripes = kv_ref.shape[0]
    stripe = lax.rem(lax.axis_index("sp"), stripes)
    blocks = query_ref.shape[0]
    block = span // blocks
    group = QUERY_HEAD_COUNT // KV_HEADS
    rows = blocks * sub

    @pl.when(tile == 0)
    def count():
        earlier = notes_ref[:, :, group:group + 1, :] < 0.5
        boundary_ref[0] = jnp.sum(earlier.astype(jnp.float32)).astype(jnp.int32)

    boundary = boundary_ref[0]
    first = tile * span
    per_tile = span // width
    taken = width // block
    zeros = jnp.zeros((rows, HD), jnp.bfloat16)
    query = query_ref[...].reshape(rows, group * HD) * jnp.bfloat16(HD ** (-0.5))
    stacked = jnp.concatenate(
        [
            jnp.concatenate([query[:, head * HD:(head + 1) * HD], zeros], axis=1)
            for head in range(group)
        ],
        axis=0,
    )
    row = lax.broadcasted_iota(jnp.int32, (rows, 1), 0)
    query_pos = first + (row // sub) * block + stripe * sub + lax.rem(row, sub)
    doc_start = jnp.where(query_pos >= boundary, boundary, 0)
    per_z = stripes // taken

    def gate_rows(index):
        block_notes = notes_ref[pl.ds(lax.rem(index, per_z) * taken, taken), index // per_z]
        return [
            jnp.concatenate(
                [block_notes[at, head:head + 1, :] for at in range(taken)], axis=1
            )
            for head in range(group)
        ]

    origin = [gate[:, 0:1] for gate in gate_rows(tile * per_tile)]
    lane = lax.broadcasted_iota(jnp.int32, (width, 2 * HD), 1)

    def chunk(index, carry, masked):
        kv = kv_ref[pl.ds(lax.rem(index, per_z) * taken, taken), index // per_z]
        kv = kv.reshape(width, 2 * HD)
        bias = [start - gate for start, gate in zip(origin, gate_rows(index))]
        if masked:
            key_pos = index * width + lax.broadcasted_iota(jnp.int32, (1, width), 1)
            allowed = (key_pos <= query_pos) & (key_pos >= doc_start)
        scores = lax.dot_general(
            stacked, kv, (((1,), (1,)), ((), ())), preferred_element_type=jnp.float32
        )
        tops, mixed = carry
        new_tops, factors, weights = [], [], []
        for head in range(group):
            score = scores[head * rows:(head + 1) * rows] + bias[head]
            if masked:
                score = jnp.where(allowed, score, MASKED)
            new_top = jnp.maximum(tops[head], jnp.max(score, axis=1, keepdims=True))
            weight = jnp.exp(score - new_top)
            factor = jnp.exp(tops[head] - new_top)
            new_tops.append(new_top)
            factors.append(factor)
            weights.append(weight.astype(jnp.bfloat16))
        mixed = mixed * jnp.concatenate(factors, axis=0) + jnp.dot(
            jnp.concatenate(weights, axis=0),
            jnp.where(lane < HD, jnp.bfloat16(1), kv),
            preferred_element_type=jnp.float32,
        )
        return (tuple(new_tops), mixed)

    carry = (
        tuple(jnp.full((rows, 1), 0.5 * MASKED, jnp.float32) for unused in range(group)),
        jnp.zeros((group * rows, 2 * HD), jnp.float32),
    )
    own = tile * per_tile
    inside = (boundary > first) & (boundary < first + span)
    second = first >= boundary
    low = jnp.where(second, boundary // width, 0)
    clean_low = jnp.where(inside, own, jnp.where(second, (boundary + width - 1) // width, 0))
    clean_low = jnp.minimum(clean_low, own)
    carry = lax.fori_loop(low, clean_low, lambda i, c: chunk(i, c, True), carry)
    carry = lax.fori_loop(clean_low, own, lambda i, c: chunk(i, c, False), carry)
    carry = lax.fori_loop(own, own + per_tile, lambda i, c: chunk(i, c, True), carry)
    unused, mixed = carry
    ratio = mixed[:, HD:] / mixed[:, :HD]
    parts = [ratio[head * rows:(head + 1) * rows] for head in range(group)]
    out_ref[...] = jnp.concatenate(parts, axis=1).astype(jnp.bfloat16).reshape(out_ref.shape)


def exchange_kernel(
    stripes,
    keys_hbm,
    values_hbm,
    query_ref,
    gates_hbm,
    documents_hbm,
    routes_hbm,
    kv_all_ref,
    got_ref,
    notes_all_ref,
    keys_ref,
    values_ref,
    gates_ref,
    documents_ref,
    routes_ref,
    notes_ref,
    kv_ref,
    l_sem,
    z_send,
    z_recv,
    p_send,
    p_recv,
    s_send,
    s_recv,
    q_send,
    q_recv,
):
    total, sub, wide = got_ref.shape
    planes = total // stripes
    chips = stripes // 2
    me = lax.axis_index("sp")
    plane, spot = me // stripes, lax.rem(me, stripes)
    chip, core = spot // 2, lax.rem(spot, 2)
    partner = plane * stripes + chip * 2 + (1 - core)
    barrier = pltpu.get_barrier_semaphore()

    def piece(other):
        head, stripe = other // stripes, lax.rem(other, stripes)
        return (
            pl.ds(pl.multiple_of(stripe * sub, sub), sub),
            pl.ds(pl.multiple_of(head * wide, wide), wide),
        )

    def greet(r, carry):
        pl.semaphore_signal(barrier, inc=1, device_id={"sp": lax.rem(me + r, total)})
        return carry

    lax.fori_loop(1, total, greet, 0)
    loads = [
        pltpu.make_async_copy(keys_hbm, keys_ref, l_sem.at[0]),
        pltpu.make_async_copy(values_hbm, values_ref, l_sem.at[1]),
        pltpu.make_async_copy(gates_hbm, gates_ref, l_sem.at[3]),
        pltpu.make_async_copy(documents_hbm, documents_ref, l_sem.at[4]),
        pltpu.make_async_copy(routes_hbm, routes_ref, l_sem.at[5]),
        pltpu.make_async_copy(query_ref.at[piece(me)], got_ref.at[me], l_sem.at[2]),
    ]
    for load in loads:
        load.start()
    for load in loads[:5]:
        load.wait()
    tok, part = keys_ref.shape[0], min(128, keys_ref.shape[0])
    group = gates_ref.shape[0] // planes
    line = lax.broadcasted_iota(jnp.int32, (part, 1), 0)
    ones = jnp.full((8, tok), 1.0, jnp.bfloat16)
    counts = []
    for g in range(planes):
        own = jnp.where(line < stripes, line + g * stripes, -1)
        hits = sum(jnp.where(own == routes_ref[k:k + 1], 1.0, 0.0) for k in range(TOP))
        count = lax.dot_general(
            ones,
            hits.astype(jnp.bfloat16),
            (((1,), (1,)), ((), ())),
            preferred_element_type=jnp.float32,
        )
        counts.append(count[:1])
    largest = functools.reduce(
        jnp.maximum, [jnp.sum(count, axis=1, keepdims=True) for count in counts]
    )
    for g in range(planes):
        notes_ref[g] = jnp.zeros(notes_ref.shape[1:], jnp.float32)
        notes_ref[g, 0:group] = gates_ref[g * group:(g + 1) * group]
        notes_ref[g, group:group + 1] = documents_ref[...].astype(jnp.float32)
        notes_ref[g, group + 1:group + 2, 0:part] = counts[g]
        notes_ref[g, group + 2:group + 3] = jnp.broadcast_to(largest, (1, tok))
    for g in range(planes):
        part = slice(g * HD, (g + 1) * HD)
        kv_ref[g] = jnp.concatenate([keys_ref[:, part], values_ref[:, part]], axis=1)
    pl.semaphore_wait(barrier, total - 1)
    sources, targets = (kv_ref, notes_ref), (kv_all_ref, notes_all_ref)

    def along(r, n):
        other = lax.rem(plane + r, planes)
        return pltpu.make_async_remote_copy(
            src_ref=sources[n].at[other],
            dst_ref=targets[n].at[spot, plane],
            send_sem=z_send.at[n, r],
            recv_sem=z_recv.at[n, r],
            device_id={"sp": other * stripes + spot},
        )

    def origin(r):
        return lax.rem(plane + planes - r, planes)

    def block(r, n):
        if r == 0:
            return sources[n].at[plane]
        return targets[n].at[spot, origin(r)]

    def across(r, m, n):
        target = lax.rem(chip + m, chips)
        return pltpu.make_async_remote_copy(
            src_ref=block(r, n),
            dst_ref=targets[n].at[spot, origin(r)],
            send_sem=p_send.at[n, r, m],
            recv_sem=p_recv.at[n, r, m],
            device_id={"sp": plane * stripes + target * 2 + core},
        )

    def over(r, m, n):
        source = lax.rem(chip + chips - m, chips) * 2 + core
        where = targets[n].at[source, origin(r)]
        return pltpu.make_async_remote_copy(
            src_ref=block(r, n) if m == 0 else where,
            dst_ref=where,
            send_sem=s_send.at[n, r, m],
            recv_sem=s_recv.at[n, r, m],
            device_id={"sp": partner},
        )

    def direct(r):
        other = lax.rem(me + r, total)
        return pltpu.make_async_remote_copy(
            src_ref=query_ref.at[piece(other)],
            dst_ref=got_ref.at[me],
            send_sem=q_send.at[r],
            recv_sem=q_recv.at[r],
            device_id={"sp": other},
        )

    both = (0, 1)
    order = sorted(range(1, planes), key=lambda r: min(r, planes - r))
    for r in order:
        for n in both:
            along(r, n).start()
    for m in range(1, chips):
        for n in both:
            across(0, m, n).start()
    for n in both:
        over(0, 0, n).start()

    def send_query(r, carry):
        direct(r).start()
        return carry

    lax.fori_loop(1, total, send_query, 0)
    kv_all_ref[spot, plane] = kv_ref[plane]
    notes_all_ref[spot, plane] = notes_ref[plane]
    loads[5].wait()
    for at, r in enumerate(order):
        for n in both:
            along(r, n).wait_recv()
            for m in range(1, chips):
                across(r, m, n).start()
            over(r, 0, n).start()
        earlier = 0 if at == 0 else order[at - 1]
        for m in range(1, chips):
            for n in both:
                across(earlier, m, n).wait_recv()
                over(earlier, m, n).start()
    for m in range(1, chips):
        for n in both:
            across(order[-1], m, n).wait_recv()
            over(order[-1], m, n).start()
    for n in both:
        for r in range(planes):
            for m in range(chips):
                over(r, m, n).wait()
        for r in range(1, planes):
            along(r, n).wait_send()
        for r in range(planes):
            for m in range(1, chips):
                across(r, m, n).wait_send()

    def end_query(r, carry):
        direct(r).wait()
        return carry

    lax.fori_loop(1, total, end_query, 0)


def exchange(operands, stripes):
    keys, values, queries, gates, documents, routes = [
        pltpu.with_memory_space_constraint(array, pltpu.HBM) for array in operands
    ]
    planes, chips = KV_HEADS, stripes // 2
    rows = -(-(QUERY_HEAD_COUNT // KV_HEADS + 3) // 8) * 8
    notes = jax.ShapeDtypeStruct((planes, rows, keys.shape[0]), jnp.float32)
    total, tok = planes * stripes, keys.shape[0]
    got = (total, tok // stripes, queries.shape[1] // planes)
    hbm = pl.BlockSpec(memory_space=pltpu.HBM)
    vmem = pl.BlockSpec(memory_space=pltpu.VMEM)
    dma = pltpu.SemaphoreType.DMA
    return pl.pallas_call(
        functools.partial(exchange_kernel, stripes),
        in_specs=[hbm] * 6,
        out_specs=[vmem] * 3,
        out_shape=[
            jax.ShapeDtypeStruct((stripes, planes, tok, 2 * HD), keys.dtype),
            jax.ShapeDtypeStruct(got, queries.dtype),
            jax.ShapeDtypeStruct((stripes,) + notes.shape, notes.dtype),
        ],
        scratch_shapes=[
            pltpu.VMEM(keys.shape, keys.dtype),
            pltpu.VMEM(values.shape, values.dtype),
            pltpu.VMEM(gates.shape, gates.dtype),
            pltpu.VMEM(documents.shape, documents.dtype),
            pltpu.VMEM(routes.shape, routes.dtype),
            pltpu.VMEM(notes.shape, notes.dtype),
            pltpu.VMEM((planes, tok, 2 * HD), keys.dtype),
            dma((6,)),
            dma((2, planes)),
            dma((2, planes)),
            dma((2, planes, chips)),
            dma((2, planes, chips)),
            dma((2, planes, chips)),
            dma((2, planes, chips)),
            dma((total,)),
            dma((total,)),
        ],
        compiler_params=pltpu.CompilerParams(
            collective_id=0, has_side_effects=True, vmem_limit_bytes=24 * 1024 * 1024
        ),
        name="exchange",
    )(keys, values, queries, gates, documents, routes)


def mixture_kernel(
    capacity,
    stripes,
    slots,
    mixed_ref,
    gain_ref,
    routes_ref,
    weights_ref,
    notes_ref,
    stream_hbm,
    project_hbm,
    gate_hbm,
    up_hbm,
    down_hbm,
    out_ref,
    stream_ref,
    begin_ref,
    rows_ref,
    project_w,
    gate_w,
    up_w,
    down_w,
    attended,
    hidden_ref,
    normed_ref,
    packed,
    landed,
    sending,
    arrived,
    inner,
    answers,
    returned,
    got,
    total,
    w_sem,
    h_send,
    h_recv,
    z_send,
    z_recv,
    a_send,
    a_recv,
    b_send,
    b_recv,
    r_send,
    r_recv,
):
    planes = notes_ref.shape[1]
    devices = planes * stripes
    tok, width = stream_ref.shape
    sub, wide = mixed_ref.shape[1:]
    backing = landed
    hidden_units = gate_w.shape[1]
    rows = stripes * slots
    step = math.gcd(width, STEP)
    me = lax.axis_index("sp")
    plane, spot = me // stripes, lax.rem(me, stripes)

    def plane_of(m):
        return 2 * lax.rem(plane // 2 + m // 2, 2) + lax.rem(plane + m, 2)

    def turned(q):
        return 2 * lax.rem((q + 1) // 2, 2) + q // 2

    barrier = pltpu.get_barrier_semaphore()

    def greet(r, carry):
        pl.semaphore_signal(barrier, inc=1, device_id={"sp": lax.rem(me + r, devices)})
        return carry

    lax.fori_loop(1, devices, greet, 0)
    weights = [
        pltpu.make_async_copy(source, target, w_sem.at[at])
        for at, (source, target) in enumerate(
            (
                (stream_hbm, stream_ref),
                (project_hbm, project_w),
                (gate_hbm.at[0], gate_w),
                (up_hbm.at[0], up_w),
                (down_hbm.at[0], down_w),
            )
        )
    ]
    for copy in weights:
        copy.start()

    def as_bf16(hit):
        return jnp.where(hit, 1.0, 0.0).astype(jnp.bfloat16)

    def iota(shape, axis):
        return lax.broadcasted_iota(jnp.int32, shape, axis)

    def exact(left, right):
        return jnp.dot(left, right, preferred_element_type=jnp.float32)

    part = min(128, tok)
    lane = iota((1, rows), 1)
    number = lax.rem(lane, slots)
    line = iota((part, rows), 0)
    same, under = as_bf16(line == lax.div(lane, slots)), as_bf16(line < lax.div(lane, slots))
    row = QUERY_HEAD_COUNT // KV_HEADS + 1
    for p in range(planes):
        told = notes_ref[spot, p][:, :part].astype(jnp.bfloat16)
        count = exact(told, same)[row:row + 1].astype(jnp.int32)
        start = exact(told, under)[row:row + 1].astype(jnp.int32)
        begin_ref[p] = jnp.where(number < count, start + number, -1)
    expert = iota((devices, 1), 0)
    earlier = as_bf16(iota((tok, tok), 0) < iota((tok, tok), 1))
    hits = [expert == routes_ref[k:k + 1] for k in range(TOP)]
    before = [exact(as_bf16(hit), earlier) for hit in hits]
    sums = [jnp.sum(jnp.where(hit, 1.0, 0.0), axis=1, keepdims=True) for hit in hits]
    high_id, low_id = iota((devices, devices), 0), iota((devices, devices), 1)
    inside = (lax.div(high_id, stripes) == lax.div(low_id, stripes)) & (low_id < high_id)
    counts = jnp.broadcast_to(sum(sums), (devices, 128)).astype(jnp.bfloat16)
    base = exact(as_bf16(inside), counts)[:, :1]
    base = base + (lax.div(expert, stripes) * rows).astype(jnp.float32)
    for k in range(TOP):
        spots = jnp.where(hits[k], before[k] + base, 0.0)
        rows_ref[k:k + 1] = jnp.sum(spots, axis=0, keepdims=True).astype(jnp.int32)
        base = base + sums[k]
    pl.semaphore_wait(barrier, devices - 1)

    def home(owner):
        head, stripe = owner // stripes, lax.rem(owner, stripes)
        return (
            pl.ds(pl.multiple_of(stripe * sub, sub), sub),
            pl.ds(pl.multiple_of(head * wide, wide), wide),
        )

    def home_copy(r):
        other = lax.rem(me + r, devices)
        return pltpu.make_async_remote_copy(
            src_ref=mixed_ref.at[other],
            dst_ref=attended.at[home(me)],
            send_sem=h_send.at[r],
            recv_sem=h_recv.at[r],
            device_id={"sp": other},
        )

    def send_home(r, carry):
        home_copy(r).start()
        return carry

    def wait_home(r, carry):
        home_copy(r).wait()
        return carry

    lax.fori_loop(1, devices, send_home, 0)
    attended[home(me)] = mixed_ref[me]
    lax.fori_loop(1, devices, wait_home, 0)
    for copy in weights[:2]:
        copy.wait()

    def project(index, squares):
        cols = pl.ds(pl.multiple_of(index * step, step), step)
        product = jnp.dot(attended[...], project_w[:, cols], preferred_element_type=jnp.float32)
        hidden = (stream_ref[:, cols].astype(jnp.float32) + product).astype(jnp.bfloat16)
        hidden_ref[:, cols] = hidden
        wider = hidden.astype(jnp.float32)
        total[:, cols] = wider
        return squares + jnp.sum(wider * wider, axis=1, keepdims=True)

    squares = lax.fori_loop(0, width // step, project, jnp.zeros((tok, 1), jnp.float32))
    inverse = lax.rsqrt(squares / width + EPS)

    def columns(body, length, size):
        def at(index, carry):
            body(pl.ds(pl.multiple_of(index * size, size), size))
            return carry

        lax.fori_loop(0, length // size, at, 0)

    def dot(left, right):
        return jnp.dot(left, right, preferred_element_type=jnp.float32)

    def norm(cols):
        scaled = hidden_ref[:, cols].astype(jnp.float32) * inverse * gain_ref[:, cols]
        normed_ref[:, cols] = scaled.astype(jnp.bfloat16)

    columns(norm, width, step)
    high_slot = lax.broadcasted_iota(jnp.int32, (capacity, 1), 0)

    def chosen_of(hit):
        return jnp.where(hit, 1.0, 0.0)

    def turned_dot(left, right):
        return lax.dot_general(
            left, right, (((0,), (0,)), ((), ())), preferred_element_type=jnp.float32
        )

    def out_copy(m):
        return pltpu.make_async_remote_copy(
            src_ref=packed.at[m],
            dst_ref=landed.at[m],
            send_sem=z_send.at[m],
            recv_sem=z_recv.at[m],
            device_id={"sp": plane_of(m) * stripes + spot},
        )

    def back_copy(m):
        return pltpu.make_async_remote_copy(
            src_ref=backing.at[m],
            dst_ref=got.at[m],
            send_sem=r_send.at[m],
            recv_sem=r_recv.at[m],
            device_id={"sp": plane_of(m) * stripes + spot},
        )

    def near_copy(source, target, send, recv, m, i):
        other = lax.rem(spot + i, stripes)
        return pltpu.make_async_remote_copy(
            src_ref=source.at[m, other],
            dst_ref=target.at[m, spot],
            send_sem=send.at[m, i],
            recv_sem=recv.at[m, i],
            device_id={"sp": plane * stripes + other},
        )

    def to_expert(m, i):
        return near_copy(sending, arrived, a_send, a_recv, m, i)

    def from_expert(m, i):
        return near_copy(answers, returned, b_send, b_recv, m, i)

    def pack(m):
        begins = plane_of(m) * rows
        hits = sum(chosen_of(rows_ref[k:k + 1] - begins == high_slot) for k in range(TOP))
        hits = hits.astype(jnp.bfloat16)

        def body(cols):
            packed[m, :, cols] = dot(hits, normed_ref[:, cols]).astype(jnp.bfloat16)

        columns(body, width, step)

    def peers(act):
        def at(i, carry):
            act(i)
            return carry

        lax.fori_loop(1, stripes, at, 0)

    def spread(m):
        hits = chosen_of(begin_ref[plane_of(m)] == high_slot).astype(jnp.bfloat16)

        @pl.when(m > 0)
        def wait():
            out_copy(m).wait_recv()

        def body(cols):
            chosen = turned_dot(hits, landed[m, :, cols]).astype(jnp.bfloat16)
            sending[m, :, :, cols] = chosen.reshape(stripes, slots, step)

        columns(body, width, step)
        arrived[m, spot] = sending[m, spot]
        peers(lambda i: to_expert(m, i).start())

    def take(m):
        peers(lambda i: to_expert(m, i).wait_recv())

    def compute(m):
        def middle(cols):
            rows_in = arrived[m].reshape(rows, width)
            gate = dot(rows_in, gate_w[:, cols])
            upper = dot(rows_in, up_w[:, cols])
            inner[:, cols] = (jax.nn.silu(gate) * upper).astype(jnp.bfloat16)

        columns(middle, hidden_units, math.gcd(hidden_units, 256))

        def last(cols):
            answer = dot(inner[...], down_w[:, cols]).astype(jnp.bfloat16)
            answers[m, :, :, cols] = answer.reshape(stripes, slots, step)

        columns(last, width, step)
        returned[m, spot] = answers[m, spot]
        peers(lambda i: from_expert(m, i).start())

    def collect(m):
        hits = chosen_of(begin_ref[plane_of(m)] == high_slot).astype(jnp.bfloat16)
        peers(lambda i: from_expert(m, i).wait_recv())

        def body(cols):
            source = returned[m, :, :, cols].reshape(rows, step)
            backing[m, :, cols] = dot(hits, source).astype(jnp.bfloat16)

        columns(body, width, step)

        @pl.when(m > 0)
        def send():
            back_copy(m).start()

    def combine(m, final):
        begins = plane_of(m) * rows
        share = sum(
            jnp.where(rows_ref[k:k + 1] - begins == high_slot, weights_ref[k:k + 1], 0.0)
            for k in range(TOP)
        )
        high = share.astype(jnp.bfloat16)
        low = (share - high.astype(jnp.float32)).astype(jnp.bfloat16)

        def body(cols):
            rows_got = got[m, :, cols]
            term = total[:, cols] + turned_dot(high, rows_got) + turned_dot(low, rows_got)
            if final:
                out_ref[:, cols] = term.astype(jnp.bfloat16)
            else:
                total[:, cols] = term

        columns(body, width, step)

    def far_first(q):
        return 2 * lax.rem(q + 1, 2) + lax.rem((q + 1) // 2, 2)

    def fill(q, carry):
        pack(far_first(q))

        @pl.when(q > 0)
        def send():
            out_copy(far_first(q - 1)).start()

        return carry

    lax.fori_loop(0, planes, fill, 0)
    landed[0] = packed[0]

    def work(q, carry):
        @pl.when((q > 0) & (q != 3))
        def first():
            collect(turned(q - 1 - q // 4))

        @pl.when(q < 3)
        def second():
            def at(extra, inner_carry):
                spread(turned(q + extra))
                take_now = turned(q)

                @pl.when(extra == 0)
                def third():
                    take(take_now)

                return inner_carry

            lax.fori_loop(0, 1 + q // 2, at, 0)

        @pl.when(q == 0)
        def ready():
            for copy in weights[2:]:
                copy.wait()

        @pl.when(q == 3)
        def last():
            take(turned(q))

        @pl.when(q < planes)
        def fourth():
            compute(turned(q))

        return carry

    lax.fori_loop(0, planes + 2, work, 0)
    got[0] = backing[0]

    def gather(q, carry):
        m = turned(q)

        @pl.when(m > 0)
        def wait():
            back_copy(m).wait_recv()

        combine(m, False)
        return carry

    lax.fori_loop(0, planes - 1, gather, 0)
    back_copy(1).wait_recv()
    combine(1, True)

    def finish_sends(m, carry):
        @pl.when(m > 0)
        def far():
            out_copy(m).wait_send()
            back_copy(m).wait_send()

        peers(lambda i: to_expert(m, i).wait_send())
        peers(lambda i: from_expert(m, i).wait_send())
        return carry

    lax.fori_loop(0, planes, finish_sends, 0)


def mixture(capacity, stripes, slots, operands):
    stream, out_weight, expert_gate, expert_up, expert_down = operands[5:]
    tok, width = stream.shape
    planes = operands[4].shape[1]
    vmem = pl.BlockSpec(memory_space=pltpu.VMEM)
    hbm = pl.BlockSpec(memory_space=pltpu.HBM)
    dma = pltpu.SemaphoreType.DMA
    block = pltpu.VMEM((planes, capacity, width), jnp.bfloat16)
    wide = pltpu.VMEM((planes, stripes, slots, width), jnp.bfloat16)
    return pl.pallas_call(
        functools.partial(mixture_kernel, capacity, stripes, slots),
        in_specs=[vmem] * 5 + [hbm] * 5,
        out_specs=vmem,
        out_shape=jax.ShapeDtypeStruct((tok, width), jnp.bfloat16),
        scratch_shapes=[
            pltpu.VMEM(stream.shape, stream.dtype),
            pltpu.VMEM((planes, 1, stripes * slots), jnp.int32),
            pltpu.VMEM((TOP, tok), jnp.int32),
            pltpu.VMEM(out_weight.shape, jnp.bfloat16),
            pltpu.VMEM(expert_gate.shape[1:], jnp.bfloat16),
            pltpu.VMEM(expert_up.shape[1:], jnp.bfloat16),
            pltpu.VMEM(expert_down.shape[1:], jnp.bfloat16),
            pltpu.VMEM((tok, out_weight.shape[0]), jnp.bfloat16),
            pltpu.VMEM((tok, width), jnp.bfloat16),
            pltpu.VMEM((tok, width), jnp.bfloat16),
            block,
            block,
            wide,
            wide,
            pltpu.VMEM((stripes * slots, expert_gate.shape[2]), jnp.bfloat16),
            wide,
            wide,
            block,
            pltpu.VMEM((tok, width), jnp.float32),
            dma((5,)),
            dma((planes * stripes,)),
            dma((planes * stripes,)),
            dma((planes,)),
            dma((planes,)),
            dma((planes, stripes)),
            dma((planes, stripes)),
            dma((planes, stripes)),
            dma((planes, stripes)),
            dma((planes,)),
            dma((planes,)),
        ],
        compiler_params=pltpu.CompilerParams(
            collective_id=1 + capacity // 8,
            has_side_effects=True,
            vmem_limit_bytes=63 * 1024 * 1024,
        ),
        name="mixture",
    )(*operands)


def fast_shards(
    queries,
    keys,
    values,
    gate_totals,
    documents,
    stream,
    out_weight,
    norm_gain,
    routes,
    route_weights,
    expert_gate,
    expert_up,
    expert_down,
):
    sp_count = lax.axis_size("sp")
    group = QUERY_HEAD_COUNT // KV_HEADS
    tok = queries.shape[0]
    stripes = sp_count // KV_HEADS
    sub = tok // stripes
    blocks = 4
    span = blocks * tok
    width = min(span, 1024)
    tiles = sp_count // blocks
    slots = max(2, 2 * tok * TOP // sp_count)
    full = stripes * slots
    kv_all, query_got, notes_all = exchange(
        (
            keys,
            values,
            queries,
            jnp.transpose(gate_totals),
            documents[None, :],
            jnp.transpose(routes),
        ),
        stripes,
    )
    worst = jnp.max(notes_all[:, :, group + 2, 0]).astype(jnp.int32)
    mixed = pl.pallas_call(
        functools.partial(attend_kernel, sub, span, width),
        grid=(tiles,),
        in_specs=[
            pl.BlockSpec((blocks, sub, group * HD), lambda i: (i, 0, 0)),
            pl.BlockSpec(kv_all.shape, lambda i: (0, 0, 0, 0)),
            pl.BlockSpec(notes_all.shape, lambda i: (0, 0, 0, 0)),
        ],
        out_specs=pl.BlockSpec((blocks, sub, group * HD), lambda i: (i, 0, 0)),
        out_shape=jax.ShapeDtypeStruct((sp_count, sub, group * HD), jnp.bfloat16),
        scratch_shapes=[pltpu.SMEM((1,), jnp.int32)],
        compiler_params=pltpu.CompilerParams(vmem_limit_bytes=48 * 1024 * 1024),
        name="attend",
    )(query_got, kv_all, notes_all)
    sizes = tuple(full * part // 32 for part in (19, 20, 21, 22, 24, 32))
    operands = (
        mixed,
        norm_gain[None, :],
        jnp.transpose(routes),
        jnp.transpose(route_weights),
        notes_all,
        stream,
        out_weight,
        expert_gate,
        expert_up,
        expert_down,
    )

    def sized(capacity):
        return lambda given: mixture(capacity, stripes, slots, given)

    choice = sum((worst > size).astype(jnp.int32) for size in sizes[:-1])
    return lax.switch(choice, [sized(size) for size in sizes], operands)


def solution(mesh):
    sp_count, tp_count = mesh.shape["sp"], mesh.shape["tp"]
    fast = tp_count == 1 and sp_count % (4 * KV_HEADS) == 0 and KV_HEADS == 4

    def body(*arrays):
        tok, stripes = arrays[0].shape[0], sp_count // KV_HEADS
        small = stripes * (2 * tok * TOP // sp_count) <= 256
        return (fast_shards if fast and small else shards)(*arrays)

    return jax.shard_map(
        body,
        mesh=mesh,
        in_specs=(
            P("sp", "tp"),
            P("sp", "tp"),
            P("sp", "tp"),
            P("sp", "tp"),
            P("sp"),
            P(("sp", "tp"), None),
            P(),
            P(),
            P(("sp", "tp"), None),
            P(("sp", "tp"), None),
            P("sp", None, "tp"),
            P("sp", None, "tp"),
            P("sp", "tp", None),
        ),
        out_specs=P(("sp", "tp"), None),
        check_vma=False,
    )
```

```python
import functools
import math

import jax
import jax.numpy as jnp
from jax import lax
from jax.experimental import pallas as pl
from jax.experimental.pallas import tpu as pltpu
from jax.sharding import PartitionSpec as P

QUERY_HEAD_COUNT = 16
KV_HEADS = 4
HD = 64
TOP = 2


EPS = 1e-06
STEP = 2048
MASKED = -1e30


def make_fold(query_rows, query_gate, key_gate_all, query_docs, first_pos, kv_local, group):
    count = query_rows.shape[0]
    scale = HD ** (-0.5)
    query_blk = query_rows.reshape(count, kv_local, group, HD)
    gate_here = query_gate.T.reshape(kv_local, group, count, 1)
    query_pos = first_pos + jnp.arange(count, dtype=jnp.int32)
    last_pos = first_pos + count - 1
    first_doc = query_docs[0]

    def block_step(carry, block_in):
        running_max, running_sum, carried = carry
        key_block, value_block, doc_block, pos_block = block_in
        width = key_block.shape[0]

        def compute(unused):
            key_heads = key_block.reshape(width, kv_local, HD)
            value_heads = value_block.reshape(width, kv_local, HD)
            gate_keys = lax.dynamic_slice_in_dim(key_gate_all, pos_block[0], width, 0).T.reshape(
                kv_local, group, 1, width
            )
            scores = (
                jnp.einsum(
                    "qkgd,nkd->kgqn", query_blk, key_heads, preferred_element_type=jnp.float32
                )
                * scale
                + gate_here
                - gate_keys
            )
            allowed = (pos_block[None, :] <= query_pos[:, None]) & (
                doc_block[None, :] == query_docs[:, None]
            )
            scores = jnp.where(allowed, scores, MASKED)
            new_max = jnp.maximum(running_max, jnp.max(scores, axis=-1))
            weights = jnp.where(allowed, jnp.exp(scores - new_max[..., None]), 0.0)
            factor = jnp.exp(running_max - new_max)
            new_sum = running_sum * factor + jnp.sum(weights, axis=-1)
            new_carried = carried * factor[..., None] + jnp.einsum(
                "kgqn,nkd->kgqd",
                weights.astype(jnp.bfloat16),
                value_heads,
                preferred_element_type=jnp.float32,
            )
            return (new_max, new_sum, new_carried)

        skipped = (pos_block[0] > last_pos) | (doc_block[width - 1] < first_doc)
        return (lax.cond(skipped, lambda unused: carry, compute, 0), None)

    def fold(carry, piece, start):
        key_piece, value_piece, doc_piece = piece
        length = key_piece.shape[0]
        width = math.gcd(length, 512)
        blocks_count = length // width
        pos_piece = jnp.arange(length, dtype=jnp.int32)
        blocks = (
            key_piece.reshape(blocks_count, width, -1),
            value_piece.reshape(blocks_count, width, -1),
            doc_piece.reshape(blocks_count, width),
            pos_piece.reshape(blocks_count, width),
        )
        carry, unused = lax.scan(block_step, carry, blocks)
        return carry

    initial = (
        jnp.full((kv_local, group, count), MASKED, jnp.float32),
        jnp.zeros((kv_local, group, count), jnp.float32),
        jnp.zeros((kv_local, group, count, HD), jnp.float32),
    )
    return (fold, initial)


def finish(running_sum, carried):
    mixed = carried / running_sum[..., None]
    count = mixed.shape[2]
    return jnp.transpose(mixed, (2, 0, 1, 3)).reshape(count, -1).astype(jnp.bfloat16)


def shards(
    queries,
    keys,
    values,
    gate_totals,
    documents,
    stream,
    out_weight,
    norm_gain,
    routes,
    route_weights,
    expert_gate,
    expert_up,
    expert_down,
):
    tp_count = lax.axis_size("tp")
    sp_count = lax.axis_size("sp")
    tp_index = lax.axis_index("tp")
    sp_index = lax.axis_index("sp")
    group = QUERY_HEAD_COUNT // KV_HEADS
    tok_local = queries.shape[0]
    own_rows = tok_local // tp_count
    first_row = sp_index * tok_local
    query_rows = lax.all_to_all(queries, "tp", split_axis=0, concat_axis=1, tiled=True)
    key_whole, value_whole = (
        lax.all_gather(keys, "tp", axis=1, tiled=True),
        lax.all_gather(values, "tp", axis=1, tiled=True),
    )
    gate_whole = lax.all_gather(gate_totals, "tp", axis=1, tiled=True)
    key_gate_all = lax.all_gather(gate_whole, "sp", axis=0, tiled=True)
    query_gate = lax.dynamic_slice_in_dim(gate_whole, tp_index * own_rows, own_rows, 0)
    query_docs = lax.dynamic_slice_in_dim(documents, tp_index * own_rows, own_rows, 0)
    fold, initial = make_fold(
        query_rows,
        query_gate,
        key_gate_all,
        query_docs,
        first_row + tp_index * own_rows,
        KV_HEADS,
        group,
    )
    running_max, running_sum, carried = fold(
        initial,
        (
            lax.all_gather(key_whole, "sp", axis=0, tiled=True),
            lax.all_gather(value_whole, "sp", axis=0, tiled=True),
            lax.all_gather(documents, "sp", axis=0, tiled=True),
        ),
        jnp.int32(0),
    )
    attended = finish(running_sum, carried)
    hidden = (
        stream.astype(jnp.float32)
        + jnp.dot(attended, out_weight, preferred_element_type=jnp.float32)
    ).astype(jnp.bfloat16)
    hidden_f = hidden.astype(jnp.float32)
    normed = (
        hidden_f
        * lax.rsqrt(jnp.mean(hidden_f * hidden_f, axis=-1, keepdims=True) + EPS)
        * norm_gain
    ).astype(jnp.bfloat16)
    local_experts = expert_gate.shape[0]
    experts_total = local_experts * sp_count
    capacity = max(2, 2 * tok_local * TOP // (tp_count * experts_total))
    flat = routes.reshape(-1)
    hits = (flat[:, None] == jnp.arange(experts_total, dtype=jnp.int32)[None, :]).astype(jnp.int32)
    slot_index = jnp.sum(jnp.cumsum(hits, axis=0) * hits, axis=1) - 1
    target = flat * capacity + slot_index
    entry_rows = jnp.repeat(normed, TOP, axis=0)
    outgoing = (
        jnp.zeros((experts_total * capacity, normed.shape[1]), jnp.bfloat16)
        .at[target]
        .set(entry_rows)
    )
    outgoing = outgoing.reshape(experts_total, capacity, -1)
    arrived = lax.all_to_all(outgoing, "sp", split_axis=0, concat_axis=0, tiled=True)
    slots = arrived.shape[1]
    both_halves = lax.all_gather(arrived, "tp", axis=0, tiled=True)
    grouped = both_halves.reshape(tp_count * sp_count, local_experts, slots, -1)
    gate = jnp.einsum("secd,edf->secf", grouped, expert_gate, preferred_element_type=jnp.float32)
    upper = jnp.einsum("secd,edf->secf", grouped, expert_up, preferred_element_type=jnp.float32)
    inner = (jax.nn.silu(gate) * upper).astype(jnp.bfloat16)
    partial_value = jnp.einsum(
        "secf,efd->secd", inner, expert_down, preferred_element_type=jnp.float32
    )
    partial_value = lax.optimization_barrier(partial_value.astype(jnp.bfloat16)).astype(jnp.float32)
    summed = lax.psum_scatter(
        partial_value.reshape(tp_count * sp_count * local_experts, slots, -1).astype(jnp.bfloat16),
        "tp",
        scatter_dimension=0,
        tiled=True,
    )
    returned = lax.all_to_all(summed, "sp", split_axis=0, concat_axis=0, tiled=True)
    answers = returned.reshape(experts_total * capacity, -1)[target].reshape(own_rows, TOP, -1)
    routed = jnp.sum(route_weights[..., None] * answers.astype(jnp.float32), axis=1)
    return (hidden_f + routed).astype(jnp.bfloat16)


def attend_kernel(sub, span, width, query_ref, kv_ref, notes_ref, out_ref, boundary_ref):
    tile = pl.program_id(0)
    stripes = kv_ref.shape[0]
    stripe = lax.rem(lax.axis_index("sp"), stripes)
    blocks = query_ref.shape[0]
    block = span // blocks
    group = QUERY_HEAD_COUNT // KV_HEADS
    rows = blocks * sub

    @pl.when(tile == 0)
    def count():
        earlier = notes_ref[:, :, group:group + 1, :] < 0.5
        boundary_ref[0] = jnp.sum(earlier.astype(jnp.float32)).astype(jnp.int32)

    boundary = boundary_ref[0]
    first = tile * span
    per_tile = span // width
    taken = width // block
    zeros = jnp.zeros((rows, HD), jnp.bfloat16)
    query = query_ref[...].reshape(rows, group * HD) * jnp.bfloat16(HD ** (-0.5))
    stacked = jnp.concatenate(
        [
            jnp.concatenate([query[:, head * HD:(head + 1) * HD], zeros], axis=1)
            for head in range(group)
        ],
        axis=0,
    )
    row = lax.broadcasted_iota(jnp.int32, (rows, 1), 0)
    query_pos = first + (row // sub) * block + stripe * sub + lax.rem(row, sub)
    doc_start = jnp.where(query_pos >= boundary, boundary, 0)
    per_z = stripes // taken

    def gate_rows(index):
        block_notes = notes_ref[pl.ds(lax.rem(index, per_z) * taken, taken), index // per_z]
        return [
            jnp.concatenate(
                [block_notes[at, head:head + 1, :] for at in range(taken)], axis=1
            )
            for head in range(group)
        ]

    origin = [gate[:, 0:1] for gate in gate_rows(tile * per_tile)]
    lane = lax.broadcasted_iota(jnp.int32, (width, 2 * HD), 1)

    def chunk(index, carry, masked):
        kv = kv_ref[pl.ds(lax.rem(index, per_z) * taken, taken), index // per_z]
        kv = kv.reshape(width, 2 * HD)
        bias = [start - gate for start, gate in zip(origin, gate_rows(index))]
        if masked:
            key_pos = index * width + lax.broadcasted_iota(jnp.int32, (1, width), 1)
            allowed = (key_pos <= query_pos) & (key_pos >= doc_start)
        scores = lax.dot_general(
            stacked, kv, (((1,), (1,)), ((), ())), preferred_element_type=jnp.float32
        )
        tops, mixed = carry
        new_tops, factors, weights = [], [], []
        for head in range(group):
            score = scores[head * rows:(head + 1) * rows] + bias[head]
            if masked:
                score = jnp.where(allowed, score, MASKED)
            new_top = jnp.maximum(tops[head], jnp.max(score, axis=1, keepdims=True))
            weight = jnp.exp(score - new_top)
            factor = jnp.exp(tops[head] - new_top)
            new_tops.append(new_top)
            factors.append(factor)
            weights.append(weight.astype(jnp.bfloat16))
        mixed = mixed * jnp.concatenate(factors, axis=0) + jnp.dot(
            jnp.concatenate(weights, axis=0),
            jnp.where(lane < HD, jnp.bfloat16(1), kv),
            preferred_element_type=jnp.float32,
        )
        return (tuple(new_tops), mixed)

    carry = (
        tuple(jnp.full((rows, 1), 0.5 * MASKED, jnp.float32) for unused in range(group)),
        jnp.zeros((group * rows, 2 * HD), jnp.float32),
    )
    own = tile * per_tile
    inside = (boundary > first) & (boundary < first + span)
    second = first >= boundary
    low = jnp.where(second, boundary // width, 0)
    clean_low = jnp.where(inside, own, jnp.where(second, (boundary + width - 1) // width, 0))
    clean_low = jnp.minimum(clean_low, own)
    carry = lax.fori_loop(low, clean_low, lambda i, c: chunk(i, c, True), carry)
    carry = lax.fori_loop(clean_low, own, lambda i, c: chunk(i, c, False), carry)
    carry = lax.fori_loop(own, own + per_tile, lambda i, c: chunk(i, c, True), carry)
    unused, mixed = carry
    ratio = mixed[:, HD:] / mixed[:, :HD]
    parts = [ratio[head * rows:(head + 1) * rows] for head in range(group)]
    out_ref[...] = jnp.concatenate(parts, axis=1).astype(jnp.bfloat16).reshape(out_ref.shape)


def exchange_kernel(
    stripes,
    keys_hbm,
    values_hbm,
    query_ref,
    gates_hbm,
    documents_hbm,
    routes_hbm,
    kv_all_ref,
    got_ref,
    notes_all_ref,
    keys_ref,
    values_ref,
    gates_ref,
    documents_ref,
    routes_ref,
    notes_ref,
    kv_ref,
    l_sem,
    z_send,
    z_recv,
    p_send,
    p_recv,
    s_send,
    s_recv,
    q_send,
    q_recv,
):
    total, sub, wide = got_ref.shape
    planes = total // stripes
    chips = stripes // 2
    me = lax.axis_index("sp")
    plane, spot = me // stripes, lax.rem(me, stripes)
    chip, core = spot // 2, lax.rem(spot, 2)
    partner = plane * stripes + chip * 2 + (1 - core)
    barrier = pltpu.get_barrier_semaphore()

    def piece(other):
        head, stripe = other // stripes, lax.rem(other, stripes)
        return (
            pl.ds(pl.multiple_of(stripe * sub, sub), sub),
            pl.ds(pl.multiple_of(head * wide, wide), wide),
        )

    def greet(r, carry):
        pl.semaphore_signal(barrier, inc=1, device_id={"sp": lax.rem(me + r, total)})
        return carry

    lax.fori_loop(1, total, greet, 0)
    loads = [
        pltpu.make_async_copy(keys_hbm, keys_ref, l_sem.at[0]),
        pltpu.make_async_copy(values_hbm, values_ref, l_sem.at[1]),
        pltpu.make_async_copy(gates_hbm, gates_ref, l_sem.at[3]),
        pltpu.make_async_copy(documents_hbm, documents_ref, l_sem.at[4]),
        pltpu.make_async_copy(routes_hbm, routes_ref, l_sem.at[5]),
        pltpu.make_async_copy(query_ref.at[piece(me)], got_ref.at[me], l_sem.at[2]),
    ]
    for load in loads:
        load.start()
    for load in loads[:5]:
        load.wait()
    tok, part = keys_ref.shape[0], min(128, keys_ref.shape[0])
    group = gates_ref.shape[0] // planes
    line = lax.broadcasted_iota(jnp.int32, (part, 1), 0)
    ones = jnp.full((8, tok), 1.0, jnp.bfloat16)
    counts = []
    for g in range(planes):
        own = jnp.where(line < stripes, line + g * stripes, -1)
        hits = sum(jnp.where(own == routes_ref[k:k + 1], 1.0, 0.0) for k in range(TOP))
        count = lax.dot_general(
            ones,
            hits.astype(jnp.bfloat16),
            (((1,), (1,)), ((), ())),
            preferred_element_type=jnp.float32,
        )
        counts.append(count[:1])
    largest = functools.reduce(
        jnp.maximum, [jnp.sum(count, axis=1, keepdims=True) for count in counts]
    )
    for g in range(planes):
        notes_ref[g] = jnp.zeros(notes_ref.shape[1:], jnp.float32)
        notes_ref[g, 0:group] = gates_ref[g * group:(g + 1) * group]
        notes_ref[g, group:group + 1] = documents_ref[...].astype(jnp.float32)
        notes_ref[g, group + 1:group + 2, 0:part] = counts[g]
        notes_ref[g, group + 2:group + 3] = jnp.broadcast_to(largest, (1, tok))
    for g in range(planes):
        part = slice(g * HD, (g + 1) * HD)
        kv_ref[g] = jnp.concatenate([keys_ref[:, part], values_ref[:, part]], axis=1)
    pl.semaphore_wait(barrier, total - 1)
    sources, targets = (kv_ref, notes_ref), (kv_all_ref, notes_all_ref)

    def along(r, n):
        other = lax.rem(plane + r, planes)
        return pltpu.make_async_remote_copy(
            src_ref=sources[n].at[other],
            dst_ref=targets[n].at[spot, plane],
            send_sem=z_send.at[n, r],
            recv_sem=z_recv.at[n, r],
            device_id={"sp": other * stripes + spot},
        )

    def origin(r):
        return lax.rem(plane + planes - r, planes)

    def block(r, n):
        if r == 0:
            return sources[n].at[plane]
        return targets[n].at[spot, origin(r)]

    def across(r, m, n):
        target = lax.rem(chip + m, chips)
        return pltpu.make_async_remote_copy(
            src_ref=block(r, n),
            dst_ref=targets[n].at[spot, origin(r)],
            send_sem=p_send.at[n, r, m],
            recv_sem=p_recv.at[n, r, m],
            device_id={"sp": plane * stripes + target * 2 + core},
        )

    def over(r, m, n):
        source = lax.rem(chip + chips - m, chips) * 2 + core
        where = targets[n].at[source, origin(r)]
        return pltpu.make_async_remote_copy(
            src_ref=block(r, n) if m == 0 else where,
            dst_ref=where,
            send_sem=s_send.at[n, r, m],
            recv_sem=s_recv.at[n, r, m],
            device_id={"sp": partner},
        )

    def direct(r):
        other = lax.rem(me + r, total)
        return pltpu.make_async_remote_copy(
            src_ref=query_ref.at[piece(other)],
            dst_ref=got_ref.at[me],
            send_sem=q_send.at[r],
            recv_sem=q_recv.at[r],
            device_id={"sp": other},
        )

    both = (0, 1)
    order = sorted(range(1, planes), key=lambda r: min(r, planes - r))
    for r in order:
        for n in both:
            along(r, n).start()
    for m in range(1, chips):
        for n in both:
            across(0, m, n).start()
    for n in both:
        over(0, 0, n).start()

    def send_query(r, carry):
        direct(r).start()
        return carry

    lax.fori_loop(1, total, send_query, 0)
    kv_all_ref[spot, plane] = kv_ref[plane]
    notes_all_ref[spot, plane] = notes_ref[plane]
    loads[5].wait()
    for at, r in enumerate(order):
        for n in both:
            along(r, n).wait_recv()
            for m in range(1, chips):
                across(r, m, n).start()
            over(r, 0, n).start()
        earlier = 0 if at == 0 else order[at - 1]
        for m in range(1, chips):
            for n in both:
                across(earlier, m, n).wait_recv()
                over(earlier, m, n).start()
    for m in range(1, chips):
        for n in both:
            across(order[-1], m, n).wait_recv()
            over(order[-1], m, n).start()
    for n in both:
        for r in range(planes):
            for m in range(chips):
                over(r, m, n).wait()
        for r in range(1, planes):
            along(r, n).wait_send()
        for r in range(planes):
            for m in range(1, chips):
                across(r, m, n).wait_send()

    def end_query(r, carry):
        direct(r).wait()
        return carry

    lax.fori_loop(1, total, end_query, 0)


def exchange(operands, stripes):
    keys, values, queries, gates, documents, routes = [
        pltpu.with_memory_space_constraint(array, pltpu.HBM) for array in operands
    ]
    planes, chips = KV_HEADS, stripes // 2
    rows = -(-(QUERY_HEAD_COUNT // KV_HEADS + 3) // 8) * 8
    notes = jax.ShapeDtypeStruct((planes, rows, keys.shape[0]), jnp.float32)
    total, tok = planes * stripes, keys.shape[0]
    got = (total, tok // stripes, queries.shape[1] // planes)
    hbm = pl.BlockSpec(memory_space=pltpu.HBM)
    vmem = pl.BlockSpec(memory_space=pltpu.VMEM)
    dma = pltpu.SemaphoreType.DMA
    return pl.pallas_call(
        functools.partial(exchange_kernel, stripes),
        in_specs=[hbm] * 6,
        out_specs=[vmem] * 3,
        out_shape=[
            jax.ShapeDtypeStruct((stripes, planes, tok, 2 * HD), keys.dtype),
            jax.ShapeDtypeStruct(got, queries.dtype),
            jax.ShapeDtypeStruct((stripes,) + notes.shape, notes.dtype),
        ],
        scratch_shapes=[
            pltpu.VMEM(keys.shape, keys.dtype),
            pltpu.VMEM(values.shape, values.dtype),
            pltpu.VMEM(gates.shape, gates.dtype),
            pltpu.VMEM(documents.shape, documents.dtype),
            pltpu.VMEM(routes.shape, routes.dtype),
            pltpu.VMEM(notes.shape, notes.dtype),
            pltpu.VMEM((planes, tok, 2 * HD), keys.dtype),
            dma((6,)),
            dma((2, planes)),
            dma((2, planes)),
            dma((2, planes, chips)),
            dma((2, planes, chips)),
            dma((2, planes, chips)),
            dma((2, planes, chips)),
            dma((total,)),
            dma((total,)),
        ],
        compiler_params=pltpu.CompilerParams(
            collective_id=0, has_side_effects=True, vmem_limit_bytes=24 * 1024 * 1024
        ),
        name="exchange",
    )(keys, values, queries, gates, documents, routes)


def mixture_kernel(
    capacity,
    stripes,
    slots,
    mixed_ref,
    gain_ref,
    routes_ref,
    weights_ref,
    notes_ref,
    stream_hbm,
    project_hbm,
    gate_hbm,
    up_hbm,
    down_hbm,
    out_ref,
    stream_ref,
    begin_ref,
    rows_ref,
    project_w,
    gate_w,
    up_w,
    down_w,
    attended,
    hidden_ref,
    normed_ref,
    packed,
    landed,
    sending,
    arrived,
    inner,
    answers,
    returned,
    got,
    total,
    w_sem,
    h_send,
    h_recv,
    z_send,
    z_recv,
    a_send,
    a_recv,
    b_send,
    b_recv,
    r_send,
    r_recv,
):
    planes = notes_ref.shape[1]
    devices = planes * stripes
    tok, width = stream_ref.shape
    sub, wide = mixed_ref.shape[1:]
    backing = landed
    hidden_units = gate_w.shape[1]
    rows = stripes * slots
    step = math.gcd(width, STEP)
    me = lax.axis_index("sp")
    plane, spot = me // stripes, lax.rem(me, stripes)

    def plane_of(m):
        return 2 * lax.rem(plane // 2 + m // 2, 2) + lax.rem(plane + m, 2)

    def turned(q):
        return 2 * lax.rem((q + 1) // 2, 2) + q // 2

    barrier = pltpu.get_barrier_semaphore()

    def greet(r, carry):
        pl.semaphore_signal(barrier, inc=1, device_id={"sp": lax.rem(me + r, devices)})
        return carry

    lax.fori_loop(1, devices, greet, 0)
    weights = [
        pltpu.make_async_copy(source, target, w_sem.at[at])
        for at, (source, target) in enumerate(
            (
                (stream_hbm, stream_ref),
                (project_hbm, project_w),
                (gate_hbm.at[0], gate_w),
                (up_hbm.at[0], up_w),
                (down_hbm.at[0], down_w),
            )
        )
    ]
    for copy in weights:
        copy.start()

    def as_bf16(hit):
        return jnp.where(hit, 1.0, 0.0).astype(jnp.bfloat16)

    def iota(shape, axis):
        return lax.broadcasted_iota(jnp.int32, shape, axis)

    def exact(left, right):
        return jnp.dot(left, right, preferred_element_type=jnp.float32)

    part = min(128, tok)
    lane = iota((1, rows), 1)
    number = lax.rem(lane, slots)
    line = iota((part, rows), 0)
    same, under = as_bf16(line == lax.div(lane, slots)), as_bf16(line < lax.div(lane, slots))
    row = QUERY_HEAD_COUNT // KV_HEADS + 1
    for p in range(planes):
        told = notes_ref[spot, p][:, :part].astype(jnp.bfloat16)
        count = exact(told, same)[row:row + 1].astype(jnp.int32)
        start = exact(told, under)[row:row + 1].astype(jnp.int32)
        begin_ref[p] = jnp.where(number < count, start + number, -1)
    expert = iota((devices, 1), 0)
    earlier = as_bf16(iota((tok, tok), 0) < iota((tok, tok), 1))
    hits = [expert == routes_ref[k:k + 1] for k in range(TOP)]
    before = [exact(as_bf16(hit), earlier) for hit in hits]
    sums = [jnp.sum(jnp.where(hit, 1.0, 0.0), axis=1, keepdims=True) for hit in hits]
    high_id, low_id = iota((devices, devices), 0), iota((devices, devices), 1)
    inside = (lax.div(high_id, stripes) == lax.div(low_id, stripes)) & (low_id < high_id)
    counts = jnp.broadcast_to(sum(sums), (devices, 128)).astype(jnp.bfloat16)
    base = exact(as_bf16(inside), counts)[:, :1]
    base = base + (lax.div(expert, stripes) * rows).astype(jnp.float32)
    for k in range(TOP):
        spots = jnp.where(hits[k], before[k] + base, 0.0)
        rows_ref[k:k + 1] = jnp.sum(spots, axis=0, keepdims=True).astype(jnp.int32)
        base = base + sums[k]
    pl.semaphore_wait(barrier, devices - 1)

    def home(owner):
        head, stripe = owner // stripes, lax.rem(owner, stripes)
        return (
            pl.ds(pl.multiple_of(stripe * sub, sub), sub),
            pl.ds(pl.multiple_of(head * wide, wide), wide),
        )

    def home_copy(r):
        other = lax.rem(me + r, devices)
        return pltpu.make_async_remote_copy(
            src_ref=mixed_ref.at[other],
            dst_ref=attended.at[home(me)],
            send_sem=h_send.at[r],
            recv_sem=h_recv.at[r],
            device_id={"sp": other},
        )

    def send_home(r, carry):
        home_copy(r).start()
        return carry

    def wait_home(r, carry):
        home_copy(r).wait()
        return carry

    lax.fori_loop(1, devices, send_home, 0)
    attended[home(me)] = mixed_ref[me]
    lax.fori_loop(1, devices, wait_home, 0)
    for copy in weights[:2]:
        copy.wait()

    def project(index, squares):
        cols = pl.ds(pl.multiple_of(index * step, step), step)
        product = jnp.dot(attended[...], project_w[:, cols], preferred_element_type=jnp.float32)
        hidden = (stream_ref[:, cols].astype(jnp.float32) + product).astype(jnp.bfloat16)
        hidden_ref[:, cols] = hidden
        wider = hidden.astype(jnp.float32)
        total[:, cols] = wider
        return squares + jnp.sum(wider * wider, axis=1, keepdims=True)

    squares = lax.fori_loop(0, width // step, project, jnp.zeros((tok, 1), jnp.float32))
    inverse = lax.rsqrt(squares / width + EPS)

    def columns(body, length, size):
        def at(index, carry):
            body(pl.ds(pl.multiple_of(index * size, size), size))
            return carry

        lax.fori_loop(0, length // size, at, 0)

    def dot(left, right):
        return jnp.dot(left, right, preferred_element_type=jnp.float32)

    def norm(cols):
        scaled = hidden_ref[:, cols].astype(jnp.float32) * inverse * gain_ref[:, cols]
        normed_ref[:, cols] = scaled.astype(jnp.bfloat16)

    columns(norm, width, step)
    high_slot = lax.broadcasted_iota(jnp.int32, (capacity, 1), 0)

    def chosen_of(hit):
        return jnp.where(hit, 1.0, 0.0)

    def turned_dot(left, right):
        return lax.dot_general(
            left, right, (((0,), (0,)), ((), ())), preferred_element_type=jnp.float32
        )

    def out_copy(m):
        return pltpu.make_async_remote_copy(
            src_ref=packed.at[m],
            dst_ref=landed.at[m],
            send_sem=z_send.at[m],
            recv_sem=z_recv.at[m],
            device_id={"sp": plane_of(m) * stripes + spot},
        )

    def back_copy(m):
        return pltpu.make_async_remote_copy(
            src_ref=backing.at[m],
            dst_ref=got.at[m],
            send_sem=r_send.at[m],
            recv_sem=r_recv.at[m],
            device_id={"sp": plane_of(m) * stripes + spot},
        )

    def near_copy(source, target, send, recv, m, i):
        other = lax.rem(spot + i, stripes)
        return pltpu.make_async_remote_copy(
            src_ref=source.at[m, other],
            dst_ref=target.at[m, spot],
            send_sem=send.at[m, i],
            recv_sem=recv.at[m, i],
            device_id={"sp": plane * stripes + other},
        )

    def to_expert(m, i):
        return near_copy(sending, arrived, a_send, a_recv, m, i)

    def from_expert(m, i):
        return near_copy(answers, returned, b_send, b_recv, m, i)

    def pack(m):
        begins = plane_of(m) * rows
        hits = sum(chosen_of(rows_ref[k:k + 1] - begins == high_slot) for k in range(TOP))
        hits = hits.astype(jnp.bfloat16)

        def body(cols):
            packed[m, :, cols] = dot(hits, normed_ref[:, cols]).astype(jnp.bfloat16)

        columns(body, width, step)

    def peers(act):
        def at(i, carry):
            act(i)
            return carry

        lax.fori_loop(1, stripes, at, 0)

    def spread(m):
        hits = chosen_of(begin_ref[plane_of(m)] == high_slot).astype(jnp.bfloat16)

        @pl.when(m > 0)
        def wait():
            out_copy(m).wait_recv()

        def body(cols):
            chosen = turned_dot(hits, landed[m, :, cols]).astype(jnp.bfloat16)
            sending[m, :, :, cols] = chosen.reshape(stripes, slots, step)

        columns(body, width, step)
        arrived[m, spot] = sending[m, spot]
        peers(lambda i: to_expert(m, i).start())

    def take(m):
        peers(lambda i: to_expert(m, i).wait_recv())

    def compute(m):
        def middle(cols):
            rows_in = arrived[m].reshape(rows, width)
            gate = dot(rows_in, gate_w[:, cols])
            upper = dot(rows_in, up_w[:, cols])
            inner[:, cols] = (jax.nn.silu(gate) * upper).astype(jnp.bfloat16)

        columns(middle, hidden_units, math.gcd(hidden_units, 512))

        def last(cols):
            answer = dot(inner[...], down_w[:, cols]).astype(jnp.bfloat16)
            answers[m, :, :, cols] = answer.reshape(stripes, slots, step)

        columns(last, width, step)
        returned[m, spot] = answers[m, spot]
        peers(lambda i: from_expert(m, i).start())

    def collect(m):
        hits = chosen_of(begin_ref[plane_of(m)] == high_slot).astype(jnp.bfloat16)
        peers(lambda i: from_expert(m, i).wait_recv())

        def body(cols):
            source = returned[m, :, :, cols].reshape(rows, step)
            backing[m, :, cols] = dot(hits, source).astype(jnp.bfloat16)

        columns(body, width, step)

        @pl.when(m > 0)
        def send():
            back_copy(m).start()

    def combine(m, final):
        begins = plane_of(m) * rows
        share = sum(
            jnp.where(rows_ref[k:k + 1] - begins == high_slot, weights_ref[k:k + 1], 0.0)
            for k in range(TOP)
        )
        high = share.astype(jnp.bfloat16)
        low = (share - high.astype(jnp.float32)).astype(jnp.bfloat16)

        def body(cols):
            rows_got = got[m, :, cols]
            term = total[:, cols] + turned_dot(high, rows_got) + turned_dot(low, rows_got)
            if final:
                out_ref[:, cols] = term.astype(jnp.bfloat16)
            else:
                total[:, cols] = term

        columns(body, width, step)

    def far_first(q):
        return 2 * lax.rem(q + 1, 2) + lax.rem((q + 1) // 2, 2)

    def fill(q, carry):
        pack(far_first(q))

        @pl.when(q > 0)
        def send():
            out_copy(far_first(q - 1)).start()

        return carry

    lax.fori_loop(0, planes, fill, 0)
    landed[0] = packed[0]

    def work(q, carry):
        @pl.when((q > 0) & (q != 3))
        def first():
            collect(turned(q - 1 - q // 4))

        @pl.when(q < 3)
        def second():
            def at(extra, inner_carry):
                spread(turned(q + extra))
                take_now = turned(q)

                @pl.when(extra == 0)
                def third():
                    take(take_now)

                return inner_carry

            lax.fori_loop(0, 1 + q // 2, at, 0)

        @pl.when(q == 0)
        def ready():
            for copy in weights[2:]:
                copy.wait()

        @pl.when(q == 3)
        def last():
            take(turned(q))

        @pl.when(q < planes)
        def fourth():
            compute(turned(q))

        return carry

    lax.fori_loop(0, planes + 2, work, 0)
    got[0] = backing[0]

    def gather(q, carry):
        m = turned(q)

        @pl.when(m > 0)
        def wait():
            back_copy(m).wait_recv()

        combine(m, False)
        return carry

    lax.fori_loop(0, planes - 1, gather, 0)
    back_copy(1).wait_recv()
    combine(1, True)

    def finish_sends(m, carry):
        @pl.when(m > 0)
        def far():
            out_copy(m).wait_send()
            back_copy(m).wait_send()

        peers(lambda i: to_expert(m, i).wait_send())
        peers(lambda i: from_expert(m, i).wait_send())
        return carry

    lax.fori_loop(0, planes, finish_sends, 0)


def mixture(capacity, stripes, slots, operands):
    stream, out_weight, expert_gate, expert_up, expert_down = operands[5:]
    tok, width = stream.shape
    planes = operands[4].shape[1]
    vmem = pl.BlockSpec(memory_space=pltpu.VMEM)
    hbm = pl.BlockSpec(memory_space=pltpu.HBM)
    dma = pltpu.SemaphoreType.DMA
    block = pltpu.VMEM((planes, capacity, width), jnp.bfloat16)
    wide = pltpu.VMEM((planes, stripes, slots, width), jnp.bfloat16)
    return pl.pallas_call(
        functools.partial(mixture_kernel, capacity, stripes, slots),
        in_specs=[vmem] * 5 + [hbm] * 5,
        out_specs=vmem,
        out_shape=jax.ShapeDtypeStruct((tok, width), jnp.bfloat16),
        scratch_shapes=[
            pltpu.VMEM(stream.shape, stream.dtype),
            pltpu.VMEM((planes, 1, stripes * slots), jnp.int32),
            pltpu.VMEM((TOP, tok), jnp.int32),
            pltpu.VMEM(out_weight.shape, jnp.bfloat16),
            pltpu.VMEM(expert_gate.shape[1:], jnp.bfloat16),
            pltpu.VMEM(expert_up.shape[1:], jnp.bfloat16),
            pltpu.VMEM(expert_down.shape[1:], jnp.bfloat16),
            pltpu.VMEM((tok, out_weight.shape[0]), jnp.bfloat16),
            pltpu.VMEM((tok, width), jnp.bfloat16),
            pltpu.VMEM((tok, width), jnp.bfloat16),
            block,
            block,
            wide,
            wide,
            pltpu.VMEM((stripes * slots, expert_gate.shape[2]), jnp.bfloat16),
            wide,
            wide,
            block,
            pltpu.VMEM((tok, width), jnp.float32),
            dma((5,)),
            dma((planes * stripes,)),
            dma((planes * stripes,)),
            dma((planes,)),
            dma((planes,)),
            dma((planes, stripes)),
            dma((planes, stripes)),
            dma((planes, stripes)),
            dma((planes, stripes)),
            dma((planes,)),
            dma((planes,)),
        ],
        compiler_params=pltpu.CompilerParams(
            collective_id=1 + capacity // 8,
            has_side_effects=True,
            vmem_limit_bytes=63 * 1024 * 1024,
        ),
        name="mixture",
    )(*operands)


def fast_shards(
    queries,
    keys,
    values,
    gate_totals,
    documents,
    stream,
    out_weight,
    norm_gain,
    routes,
    route_weights,
    expert_gate,
    expert_up,
    expert_down,
):
    sp_count = lax.axis_size("sp")
    group = QUERY_HEAD_COUNT // KV_HEADS
    tok = queries.shape[0]
    stripes = sp_count // KV_HEADS
    sub = tok // stripes
    blocks = 4
    span = blocks * tok
    width = min(span, 1024)
    tiles = sp_count // blocks
    slots = max(2, 2 * tok * TOP // sp_count)
    full = stripes * slots
    kv_all, query_got, notes_all = exchange(
        (
            keys,
            values,
            queries,
            jnp.transpose(gate_totals),
            documents[None, :],
            jnp.transpose(routes),
        ),
        stripes,
    )
    worst = jnp.max(notes_all[:, :, group + 2, 0]).astype(jnp.int32)
    mixed = pl.pallas_call(
        functools.partial(attend_kernel, sub, span, width),
        grid=(tiles,),
        in_specs=[
            pl.BlockSpec((blocks, sub, group * HD), lambda i: (i, 0, 0)),
            pl.BlockSpec(kv_all.shape, lambda i: (0, 0, 0, 0)),
            pl.BlockSpec(notes_all.shape, lambda i: (0, 0, 0, 0)),
        ],
        out_specs=pl.BlockSpec((blocks, sub, group * HD), lambda i: (i, 0, 0)),
        out_shape=jax.ShapeDtypeStruct((sp_count, sub, group * HD), jnp.bfloat16),
        scratch_shapes=[pltpu.SMEM((1,), jnp.int32)],
        compiler_params=pltpu.CompilerParams(vmem_limit_bytes=48 * 1024 * 1024),
        name="attend",
    )(query_got, kv_all, notes_all)
    sizes = tuple(full * part // 32 for part in (20, 22, 24, 32))
    operands = (
        mixed,
        norm_gain[None, :],
        jnp.transpose(routes),
        jnp.transpose(route_weights),
        notes_all,
        stream,
        out_weight,
        expert_gate,
        expert_up,
        expert_down,
    )

    def sized(capacity):
        return lambda given: mixture(capacity, stripes, slots, given)

    choice = sum((worst > size).astype(jnp.int32) for size in sizes[:-1])
    return lax.switch(choice, [sized(size) for size in sizes], operands)


def solution(mesh):
    sp_count, tp_count = mesh.shape["sp"], mesh.shape["tp"]
    fast = tp_count == 1 and sp_count % (4 * KV_HEADS) == 0 and KV_HEADS == 4

    def body(*arrays):
        tok, stripes = arrays[0].shape[0], sp_count // KV_HEADS
        small = stripes * (2 * tok * TOP // sp_count) <= 256
        return (fast_shards if fast and small else shards)(*arrays)

    return jax.shard_map(
        body,
        mesh=mesh,
        in_specs=(
            P("sp", "tp"),
            P("sp", "tp"),
            P("sp", "tp"),
            P("sp", "tp"),
            P("sp"),
            P(("sp", "tp"), None),
            P(),
            P(),
            P(("sp", "tp"), None),
            P(("sp", "tp"), None),
            P("sp", None, "tp"),
            P("sp", None, "tp"),
            P("sp", "tp", None),
        ),
        out_specs=P(("sp", "tp"), None),
        check_vma=False,
    )
```
